256 devices in a mesh: rep: 2 (over z_hi), fs: 16 (over z_lo, x), tp: 8 (over y, core).
Axes of the slice: x: 4, y: 4, z: 8 (z_hi: 2, z_lo: 4; z = z_hi * 4 + z_lo), core: 2. Of those that a mesh axis runs over, the one named last changes fastest.
Arguments:
- stream: bfloat16 [32768, 2048], P(('rep', 'fs', 'tp')), may hold values from -6 to 6
- gate_weight: bfloat16 [2048, 2816], P('fs', 'tp'), may hold values from -0.125 to 0.125
- up_weight: bfloat16 [2048, 2816], P('fs', 'tp'), may hold values from -0.125 to 0.125
- down_weight: bfloat16 [2816, 2048], P('tp', 'fs'), may hold values from -0.21875 to 0.21875
- query_weight: bfloat16 [2048, 512], P('fs', 'tp'), may hold values from -0.125 to 0.125
- key_weight: bfloat16 [2048, 512], P('fs', 'tp'), may hold values from -0.125 to 0.125
- value_weight: bfloat16 [2048, 1024], P('fs', 'tp'), may hold values from -0.125 to 0.125
- outgate_weight: bfloat16 [2048, 1024], P('fs', 'tp'), may hold values from -0.125 to 0.125
- decay_down: bfloat16 [2048, 32], replicated, may hold values from -0.125 to 0.125
- decay_up: bfloat16 [32, 512], P(None, 'tp'), may hold values from -2 to 2
- decay_bias: float32 [512], P('tp'), may hold values from -0.5 to 7
- head_gain: float32 [128], replicated, may hold values from 0.1 to 1.9
- out_weight: bfloat16 [1024, 2048], P('tp', 'fs'), may hold values from -0.375 to 0.375
- norm_gain: float32 [3, 2048], replicated, may hold values from 0.1 to 1.9
Outputs:
- layer_out: bfloat16 [32768, 2048], P(('rep', 'fs', 'tp'))
The draws below stay inside these ranges and needn't reach their ends.
All inputs are finite; a program needn't handle non-finite values.
Results may differ from the reference program's by a relative error of at most 0.015.
Values may be sent and summed in bfloat16 or wider, within the bound.
A program may use at most 128 MiB of HBM per device.

```python
import jax
import jax.numpy as jnp
from jax import lax

D = 2048
FF = 2816
HEADS = 8
DK = 64
DV = 128
GR = 32
BLOCK = 64
KW = 512
VW = 1024
SEQLEN = 1024
SEQS = 32
TOKENS = 32768


def draw_decay_bias(key, part):
    pick_key, fast_key, slow_key = jax.random.split(key, 3)
    share = 0.5
    quick = jax.random.uniform(pick_key, (HEADS, 1), jnp.float32) < share
    fast_values = jax.random.uniform(fast_key, (HEADS, DK), jnp.float32, -0.5, 1.5)
    slow_values = jax.random.uniform(slow_key, (HEADS, DK), jnp.float32, 4.0, 7.0)
    return jnp.where(quick, fast_values, slow_values).reshape(HEADS * DK)


def shard_levels(rng, extent, cuts, least, top_value):
    gain, own = 1.0, jax.random.fold_in(rng, 6)
    for axis_at, parts in cuts:
        steps = jnp.exp(jax.random.uniform(jax.random.fold_in(own, axis_at), (parts,), jnp.float32, least / len(cuts), top_value / len(cuts)))
        gain = gain * jnp.repeat(steps, extent[axis_at] // parts).reshape([-1 if axis == axis_at else 1 for axis in range(len(extent))])
    return gain


def scatter_about(own_key, dims, width, reach, cuts=(), kind=jnp.bfloat16):
    entries = width * jax.random.normal(own_key, dims, jnp.float32)
    if cuts:
        entries = entries * shard_levels(own_key, dims, cuts, -0.22, 0.18)
    return jnp.clip(entries, -reach, reach).astype(kind)


def setup_inputs(seed: int = 0) -> dict:
    arg_keys = jax.random.split(jax.random.key(seed), 15)
    return {
        "stream": scatter_about(arg_keys[0], (TOKENS, D), 1.0, 6.0, ((0, 256),)),
        "gate_weight": scatter_about(arg_keys[1], (D, FF), D ** -0.5, 0.125, ((0, 16), (1, 8))),
        "up_weight": scatter_about(arg_keys[2], (D, FF), D ** -0.5, 0.125, ((0, 16), (1, 8))),
        "down_weight": scatter_about(arg_keys[3], (FF, D), (FF // 4) ** -0.5, 0.21875, ((0, 8), (1, 16))),
        "query_weight": scatter_about(arg_keys[4], (D, KW), D ** -0.5, 0.125, ((0, 16), (1, 8))),
        "key_weight": scatter_about(arg_keys[5], (D, KW), D ** -0.5, 0.125, ((0, 16), (1, 8))),
        "value_weight": scatter_about(arg_keys[6], (D, VW), D ** -0.5, 0.125, ((0, 16), (1, 8))),
        "outgate_weight": scatter_about(arg_keys[7], (D, VW), D ** -0.5, 0.125, ((0, 16), (1, 8))),
        "decay_down": scatter_about(arg_keys[8], (D, GR), D ** -0.5, 0.125),
        "decay_up": scatter_about(arg_keys[9], (GR, KW), (GR // 4) ** -0.5, 2.0, ((1, 8),)),
        "decay_bias": draw_decay_bias(jax.random.fold_in(arg_keys[14], 71), 0),
        "head_gain": jnp.clip(1.0 + 0.18 * jax.random.normal(arg_keys[11], (DV,), jnp.float32), 0.1, 1.9),
        "out_weight": scatter_about(arg_keys[12], (VW, D), (VW // 4) ** -0.5, 0.375, ((0, 8), (1, 16))),
        "norm_gain": jnp.clip(1.0 + 0.18 * jax.random.normal(arg_keys[13], (3, D), jnp.float32), 0.1, 1.9),
    }


RESIDUAL_SCALE = 2.0 ** 0.5
BRANCH_SCALE = 0.5
NORM_EPS = 1e-05
HEAD_EPS = 0.01
GATE_DIVISOR = 16.0

def layer_norm(values, norm_scale):
    average = lax.optimization_barrier(jnp.mean(values, -1, keepdims=True))
    centred = values - average
    spread = lax.optimization_barrier(jnp.mean(centred * centred, -1, keepdims=True))
    return (centred * lax.rsqrt(spread + NORM_EPS) * norm_scale).astype(jnp.bfloat16)

def blocked_mixer(query, key_rows, value_rows, log_gate):
    length, head_count, key_dim = query.shape
    value_dim = value_rows.shape[2]
    block_count = length // BLOCK
    highest = lax.Precision.HIGHEST

    def split_blocks(values):
        return values.reshape(block_count, BLOCK, head_count, values.shape[2]).transpose(0, 2, 1, 3)
    causal = jnp.tril(jnp.ones((BLOCK, BLOCK), dtype=bool))

    def advance(carried, inputs):
        query_blk, key_blk, value_blk, decay_blk = inputs
        log_gaps = decay_blk[:, :, None, :] - decay_blk[:, None, :, :]
        log_gaps = jnp.where(causal[None, :, :, None], log_gaps, -jnp.inf)
        scores = lax.optimization_barrier(jnp.sum(query_blk[:, :, None, :] * key_blk[:, None, :, :] * jnp.exp(log_gaps), axis=-1))
        inside = jnp.einsum('hij,hjv->hiv', scores, value_blk, precision=highest)
        carried_part = jnp.einsum('hid,hdv->hiv', query_blk * jnp.exp(decay_blk), carried, precision=highest)
        closing = decay_blk[:, -1, :]
        update = jnp.einsum('hjd,hjv->hdv', key_blk * jnp.exp(closing[:, None, :] - decay_blk), value_blk, precision=highest)
        return (carried * jnp.exp(closing)[:, :, None] + update, inside + carried_part)
    cumulative = jnp.cumsum(split_blocks(log_gate), axis=2)
    start_state = jnp.zeros((head_count, key_dim, value_dim), jnp.float32)
    _, outputs = lax.scan(advance, start_state, (split_blocks(query), split_blocks(key_rows), split_blocks(value_rows), cumulative))
    return outputs.transpose(0, 2, 1, 3).reshape(length, head_count, value_dim)

def reference(stream, gate_weight, up_weight, down_weight, query_weight, key_weight, value_weight, outgate_weight, decay_down, decay_up, decay_bias, head_gain, out_weight, norm_gain):

    def ffn_half(current, norm_scale):
        gate = jnp.dot(current, gate_weight, preferred_element_type=jnp.float32)
        upward = jnp.dot(current, up_weight, preferred_element_type=jnp.float32)
        hidden = (jax.nn.silu(gate) * upward).astype(jnp.bfloat16)
        summed = jnp.dot(hidden, down_weight, preferred_element_type=jnp.float32)
        return layer_norm(RESIDUAL_SCALE * current.astype(jnp.float32) + BRANCH_SCALE * summed, norm_scale)

    def one_sequence(sequence):
        first = ffn_half(sequence, norm_gain[0])
        query = jnp.dot(first, query_weight, preferred_element_type=jnp.float32).astype(jnp.bfloat16)
        key_rows = jnp.dot(first, key_weight, preferred_element_type=jnp.float32).astype(jnp.bfloat16)
        value_rows = jnp.dot(first, value_weight, preferred_element_type=jnp.float32).astype(jnp.bfloat16)
        outgate = jnp.dot(first, outgate_weight, preferred_element_type=jnp.float32).astype(jnp.bfloat16)
        low_rank = jnp.dot(first, decay_down, preferred_element_type=jnp.float32).astype(jnp.bfloat16)
        pre_gate = jnp.dot(low_rank, decay_up, preferred_element_type=jnp.float32) + decay_bias
        log_gate = jax.nn.log_sigmoid(pre_gate) / GATE_DIVISOR
        length = first.shape[0]
        mixed = blocked_mixer(query.astype(jnp.float32).reshape(length, HEADS, DK) * DK ** (-0.5), key_rows.astype(jnp.float32).reshape(length, HEADS, DK), value_rows.astype(jnp.float32).reshape(length, HEADS, DV), log_gate.reshape(length, HEADS, DK))
        normed = mixed * lax.rsqrt(lax.optimization_barrier(jnp.mean(mixed * mixed, -1, keepdims=True)) + HEAD_EPS) * head_gain
        gated = (normed.reshape(length, HEADS * DV) * jax.nn.silu(outgate.astype(jnp.float32))).astype(jnp.bfloat16)
        summed = jnp.dot(gated, out_weight, preferred_element_type=jnp.float32)
        second = layer_norm(RESIDUAL_SCALE * first.astype(jnp.float32) + summed, norm_gain[1])
        return ffn_half(second, norm_gain[2])
    sequences = stream.reshape(SEQS, SEQLEN, D)
    return lax.map(one_sequence, sequences).reshape(TOKENS, D)
```

```python
import functools

import jax
import jax.numpy as jnp
from jax import lax
from jax.experimental import pallas as pl
from jax.experimental.pallas import tpu as pltpu
from jax.sharding import PartitionSpec as P

MESH = pl.DeviceIdType.MESH
F32, BF16 = jnp.float32, jnp.bfloat16
D, DK, DV, GR = 2048, 64, 128, 32
ROWS = 128
HID = 352
CHUNKS = ((0, 96, 192), (192, 272, 352))
PROJ = 384
BLK = 128
RESIDUAL_SCALE = 2.0**0.5
BRANCH_SCALE = 0.5
NORM_EPS = 1e-05
HEAD_EPS = 0.01
GATE_DIVISOR = 16.0

NT = (((1,), (1,)), ((), ()))
NN = (((1,), (0,)), ((), ()))
TN = (((0,), (0,)), ((), ()))


def dot(a, b, dims=NN, **kw):
    return lax.dot_general(a, b, dims, preferred_element_type=F32, **kw)


def place():
    r, f, t = lax.axis_index("rep"), lax.axis_index("fs"), lax.axis_index("tp")
    return r, f // 4, f % 4, t // 2, t % 2


def neighbour(dim, step):
    r, zl, x, y, c = place()
    if dim == "x":
        return (r, zl * 4 + (x + step + 4) % 4, y * 2 + c)
    if dim == "y":
        return (r, zl * 4 + x, ((y + step + 4) % 4) * 2 + c)
    if dim == "c":
        return (r, zl * 4 + x, y * 2 + 1 - c)
    z = (r * 4 + zl + step + 8) % 8
    return (z // 4, (z % 4) * 4 + x, y * 2 + c)


class Gather:
    def __init__(self, order, at, rows, send, recv, pending):
        self.order, self.at, self.rows = order, at, rows
        self.send, self.recv, self.pending = send, recv, pending
        r, zl, x, y, c = place()
        self.pos = {"x": x, "y": y, "z": zl}

    def region(self, phase, shift, lo, hi):
        idx = {}
        for k, dim in enumerate(self.order):
            if k < phase:
                idx[dim] = slice(None)
            elif k == phase:
                idx[dim] = (self.pos[dim] + shift) % 4
            else:
                idx[dim] = self.pos[dim]
        return self.at(idx, pl.ds(lo, hi - lo))

    def copy(self, phase, shift, part, stage, way):
        lo, mid, hi = self.rows
        lo, hi = ((lo, hi), (lo, mid), (mid, hi))[part]
        region = self.region(phase, shift, lo, hi)
        return pltpu.make_async_remote_copy(
            src_ref=region,
            dst_ref=region,
            send_sem=self.send(phase, stage, way),
            recv_sem=self.recv(phase, stage, way),
            device_id=neighbour(self.order[phase], 1 if way == 0 else -1),
            device_id_type=MESH,
        )

    def begin(self, phase):
        for way in (0, 1):
            cp = self.copy(phase, 0, 0, 0, way)
            cp.start()
            self.pending.append(cp)

    def pass_on(self, phase):
        for way in (0, 1):
            self.copy(phase, 3 if way == 0 else 1, 0, 0, way).wait_recv()
        for way in (0, 1):
            cp = self.copy(phase, 3 if way == 0 else 1, way + 1, 1, way)
            cp.start()
            self.pending.append(cp)

    def finish(self, phase):
        for way in (0, 1):
            self.copy(phase, 2, way + 1, 1, way).wait_recv()


def layer_norm(values, norm_scale):
    average = jnp.mean(values, -1, keepdims=True)
    centred = values - average
    spread = jnp.mean(centred * centred, -1, keepdims=True)
    return (centred * lax.rsqrt(spread + NORM_EPS) * norm_scale).astype(BF16)


def silu(v):
    return v / (1.0 + jnp.exp(-v))


def kernel(
    stop,
    x_ref, g_ref, u_ref, d_ref, q_ref, k_ref, v_ref, og_ref, dd_ref, du_ref, bias_ref, gain_ref, wo_ref, norm_ref,
    out_ref,
    W, Wa, Wo, WaW, xa, xb, hidT, hid, acc, part, fa, proj, gout, gin,
    lsem, fsend, frecv, asend, arecv, osend, orecv, csend, crecv, ysend, yrecv,
):
    r, zl, x, y, c = place()
    t = y * 2 + c
    barrier = pltpu.get_barrier_semaphore()
    for dim in "xyz":
        for step in (1, -1):
            pl.semaphore_signal(barrier, 1, device_id=neighbour(dim, step), device_id_type=MESH)
    pl.semaphore_signal(barrier, 1, device_id=neighbour("c", 1), device_id_type=MESH)
    pl.semaphore_signal(barrier, 1, device_id=neighbour("y", 2), device_id_type=MESH)
    own = []
    for w, ref in enumerate((g_ref, u_ref, d_ref)):
        own.append(pltpu.make_async_copy(ref, W.at[w, y, zl, x], lsem.at[w]))
    own.append(pltpu.make_async_copy(wo_ref, Wo.at[y, zl, x], lsem.at[3]))
    own.append(pltpu.make_async_copy(x_ref, xa.at[c], lsem.at[4]))
    for cp in own:
        cp.start()
    pl.semaphore_wait(barrier, 8)
    for cp in own:
        cp.wait()

    pending = []

    def across(src, dst, slot):
        return pltpu.make_async_remote_copy(
            src_ref=src, dst_ref=dst, send_sem=csend.at[slot], recv_sem=crecv.at[slot],
            device_id=neighbour("c", 1), device_id_type=MESH,
        )

    def swap(src, dst, slot):
        cp = across(src, dst, slot)
        cp.start()
        pending.append(cp)

    orders = (("x", "z", "y"), ("z", "y", "x"), ("y", "x", "z"))

    def ffn_gather(ch, w):
        return Gather(
            orders[w],
            lambda idx, rows: W.at[w, idx["y"], idx["z"], idx["x"], rows],
            CHUNKS[ch],
            lambda ph, st, way: fsend.at[ch, w, ph, st, way],
            lambda ph, st, way: frecv.at[ch, w, ph, st, way],
            pending,
        )

    ffn = [[ffn_gather(ch, w) for w in range(3)] for ch in range(2)]

    for w in range(3):
        ffn[0][w].begin(0)
    swap(xa.at[c], xa.at[c], 0)
    for w in range(3):
        ffn[1][w].begin(0)
    Wa[zl, x, 0:64, :] = q_ref[...]
    Wa[zl, x, 64:128, :] = k_ref[...]
    Wa[zl, x, 128:256, :] = v_ref[...].astype(F32).T.astype(BF16)
    Wa[zl, x, 256:384, :] = og_ref[...].astype(F32).T.astype(BF16)

    for ph in range(3):
        if ph:
            for ch in range(2):
                for w in range(3):
                    ffn[ch][w].finish(ph - 1)
                    ffn[ch][w].begin(ph)
        for ch in range(2):
            for w in range(3):
                ffn[ch][w].pass_on(ph)

    def hidden(ch, rows):
        lo, _, hi = CHUNKS[ch]
        size = hi - lo

        def body(yy, _):
            both = rows[...].reshape(2 * ROWS, D)
            gate, up = (
                dot(
                    jnp.concatenate(
                        [W[w, yy, f // 4, f % 4, lo:hi, :] for f in range(16)], axis=1
                    ),
                    both,
                    NT,
                )
                for w in (0, 1)
            )
            hidT[pl.ds(pl.multiple_of(yy * size, 16), size), :] = silu(gate) * up
            return 0

        lax.fori_loop(0, 4, body, 0)
        hid[:, : 4 * size] = hidT[: 4 * size, :].T.astype(BF16)

    def down(ch):
        lo, _, hi = CHUNKS[ch]
        size = hi - lo

        def body(j, _):
            weights = jnp.concatenate(
                [
                    jnp.concatenate([W[2, yy, j // 2, (j % 2) * 2 + i, lo:hi, :] for i in range(2)], axis=1)
                    for yy in range(4)
                ],
                axis=0,
            )
            cols = pl.ds(pl.multiple_of(j * 256, 256), 256)
            term = dot(hid[:, : 4 * size], weights)
            for half in range(2):
                piece = term[half * ROWS : (half + 1) * ROWS]
                if ch:
                    acc[half, :, cols] += piece
                else:
                    acc[half, :, cols] = piece
            return 0

        lax.fori_loop(0, 8, body, 0)

    def joined(slot, residual, scale, branch, norm):
        across(acc.at[c], part.at[slot], 2 + slot).wait_recv()
        total = acc[c] + part[slot]
        return layer_norm(scale * residual.astype(F32) + branch * total, norm_ref[norm : norm + 1, :])

    for ch in range(2):
        if ch == 0:
            across(xa.at[c], xa.at[c], 0).wait_recv()
        for w in range(3):
            ffn[ch][w].finish(2)
        hidden(ch, xa)
        down(ch)
    swap(acc.at[1 - c], part.at[0], 2)
    first = joined(0, xa[c], RESIDUAL_SCALE, BRANCH_SCALE, 0)
    fa[t] = first
    if stop == 1:
        out_ref[...] = fa[t]

    if stop != 1:
        def along(block, rows, slot, step):
            ref = fa.at[block, rows]
            return pltpu.make_async_remote_copy(
                src_ref=ref, dst_ref=ref, send_sem=ysend.at[slot], recv_sem=yrecv.at[slot],
                device_id=neighbour("y", step), device_id_type=MESH,
            )

        def go(cp):
            cp.start()
            pending.append(cp)

        every, low_half, high_half = pl.ds(0, ROWS), pl.ds(0, ROWS // 2), pl.ds(ROWS // 2, ROWS // 2)
        go(along(t, every, 0, 1))
        go(along(t, every, 1, -1))
        swap(fa.at[t], fa.at[t], 5)
        ga = Gather(
            ("x", "z"), lambda idx, rows: Wa.at[idx["z"], idx["x"], rows], (0, 192, 384),
            lambda ph, st, way: asend.at[ph, st, way], lambda ph, st, way: arecv.at[ph, st, way], pending,
        )
        go_ = Gather(
            ("y", "z", "x"), lambda idx, rows: Wo.at[idx["y"], idx["z"], idx["x"], rows], (0, 64, 128),
            lambda ph, st, way: osend.at[ph, st, way], lambda ph, st, way: orecv.at[ph, st, way], pending,
        )
        ga.begin(0)
        go_.begin(0)
        ga.pass_on(0)
        go_.pass_on(0)
        ga.finish(0)
        ga.begin(1)
        go_.finish(0)
        go_.begin(1)
        ga.pass_on(1)
        go_.pass_on(1)
        go_.finish(1)
        go_.begin(2)
        ga.finish(1)

        left, right, far = ((y + 3) % 4) * 2, ((y + 1) % 4) * 2, ((y + 2) % 4) * 2

        def widen(f, _):
            WaW[0:PROJ, pl.ds(pl.multiple_of(f * 128, 128), 128)] = Wa[f // 4, f % 4]
            return 0

        lax.fori_loop(0, 16, widen, 0)
        WaW[PROJ : PROJ + GR, :] = dd_ref[...]

        def project(pair):
            rows = fa[pl.ds(pair, 2)].reshape(2 * ROWS, D)
            proj[pl.ds(pl.multiple_of(pair * ROWS, 256), 256), 0 : PROJ + GR] = dot(rows, WaW[...], NT)

        across(fa.at[t], fa.at[t + 1 - 2 * c], 5).wait_recv()
        project(y * 2)
        along(left + c, every, 0, 1).wait_recv()
        go(along(left + c, low_half, 2, 1))
        swap(fa.at[left + c], fa.at[left + c], 6)
        along(right + c, every, 1, -1).wait_recv()
        go(along(right + c, high_half, 3, -1))
        swap(fa.at[right + c], fa.at[right + c], 7)
        go_.pass_on(2)
        across(fa.at[left + 1 - c], fa.at[left + 1 - c], 6).wait_recv()
        project(left)
        across(fa.at[right + 1 - c], fa.at[right + 1 - c], 7).wait_recv()
        project(right)
        along(far + c, low_half, 2, 1).wait_recv()
        along(far + c, high_half, 3, -1).wait_recv()
        swap(fa.at[far + c], fa.at[far + c], 8)
        across(fa.at[far + 1 - c], fa.at[far + 1 - c], 8).wait_recv()
        project(far)

        rowi = lax.broadcasted_iota(jnp.int32, (BLK, BLK), 0)
        coli = lax.broadcasted_iota(jnp.int32, (BLK, BLK), 1)
        tri = (rowi >= coli).astype(F32)

        def middle(b, size):
            if size >= 8:
                v = b.reshape(BLK // (2 * size), 2 * size, DK)[:, size - 1 : size, :]
                return jnp.broadcast_to(v, (BLK // (2 * size), 2 * size, DK)).reshape(BLK, DK)
            v = b.reshape(BLK // 8, 8, DK)
            sub = lax.broadcasted_iota(jnp.int32, (BLK // 8, 8, DK), 1)
            out = None
            for seg in range(8 // (2 * size)):
                at = seg * 2 * size + size - 1
                here = jnp.broadcast_to(v[:, at : at + 1, :], (BLK // 8, 8, DK))
                out = here if out is None else jnp.where(sub >= seg * 2 * size, here, out)
            return out.reshape(BLK, DK)

        def mix(i, state):
            rows = pl.ds(pl.multiple_of(i * BLK, BLK), BLK)
            p = proj[rows, :].astype(BF16)
            q = p[:, 0:64].astype(F32) * DK**-0.5
            k = p[:, 64:128].astype(F32)
            v = p[:, 128:256]
            pre = dot(p[:, PROJ : PROJ + GR], du_ref[...]) + bias_ref[...]
            lg = (jnp.minimum(pre, 0.0) - jnp.log1p(jnp.exp(-jnp.abs(pre)))) / GATE_DIVISOR
            b = dot(tri, lg, precision=lax.Precision.HIGHEST)
            scores = jnp.where(rowi == coli, jnp.sum(q * k, axis=1, keepdims=True), 0.0)
            size = 1
            while size < BLK:
                e = jnp.exp(-jnp.abs(b - middle(b, size)))
                s = dot((q * e).astype(BF16), (k * e).astype(BF16), NT)
                mask = (
                    (rowi // (2 * size) == coli // (2 * size))
                    & (rowi % (2 * size) >= size)
                    & (coli % (2 * size) < size)
                )
                scores = scores + jnp.where(mask, s, 0.0)
                size *= 2
            mixed = dot(scores.astype(BF16), v)
            mixed = mixed + dot((q * jnp.exp(b)).astype(BF16), state.astype(BF16), NT)
            last = b[BLK - 1 : BLK, :]
            state = state * jnp.exp(last) + dot(v, (k * jnp.exp(last - b)).astype(BF16), TN)
            normed = mixed * lax.rsqrt(jnp.mean(mixed * mixed, -1, keepdims=True) + HEAD_EPS) * gain_ref[...]
            gout[rows, :] = (normed * silu(p[:, 256:384].astype(F32))).astype(BF16)
            return state

        lax.fori_loop(0, 8, mix, jnp.zeros((DV, DK), F32))

        def home(step):
            to = (y + step) % 4
            return pltpu.make_async_remote_copy(
                src_ref=gout.at[pl.ds(pl.multiple_of(to * 256, 256), 256)], dst_ref=gin.at[y],
                send_sem=ysend.at[3 + step], recv_sem=yrecv.at[3 + step],
                device_id=neighbour("y", step), device_id_type=MESH,
            )

        for step in (2, 1, 3):
            go(home(step))
        gin[y] = gout[pl.ds(pl.multiple_of(y * 256, 256), 256), :]
        go_.finish(2)
        for step in (1, 3, 2):
            cp = pltpu.make_async_remote_copy(
                src_ref=gout.at[pl.ds(0, 256)], dst_ref=gin.at[(y + 4 - step) % 4],
                send_sem=ysend.at[3 + step], recv_sem=yrecv.at[3 + step],
                device_id=neighbour("y", step), device_id_type=MESH,
            )
            cp.wait_recv()

        def out_proj(j, _):
            weights = jnp.concatenate(
                [
                    jnp.concatenate([Wo[yy, j // 2, (j % 2) * 2 + i] for i in range(2)], axis=1)
                    for yy in range(4)
                ],
                axis=0,
            )
            cols = pl.ds(pl.multiple_of(j * 256, 256), 256)
            term = dot(jnp.concatenate([gin[yy] for yy in range(4)], axis=1), weights)
            acc[0, :, cols] = term[:ROWS]
            acc[1, :, cols] = term[ROWS:]
            return 0

        for cp in pending:
            cp.wait_send()
        pending.clear()
        lax.fori_loop(0, 8, out_proj, 0)
        swap(acc.at[1 - c], part.at[1], 3)
        xb[c] = joined(1, fa[t], RESIDUAL_SCALE, 1.0, 1)
        if stop == 2:
            out_ref[...] = xb[c]
        else:
            swap(xb.at[c], xb.at[c], 1)
            across(xb.at[1 - c], xb.at[1 - c], 1).wait_recv()
            for cp in pending:
                cp.wait_send()
            pending.clear()
            for ch in range(2):
                hidden(ch, xb)
                down(ch)
            swap(acc.at[1 - c], part.at[2], 4)
            out_ref[...] = joined(2, xb[c], RESIDUAL_SCALE, BRANCH_SCALE, 2)
    for cp in pending:
        cp.wait_send()


def on_device(
    stop, stream, gate_weight, up_weight, down_weight, query_weight, key_weight, value_weight, outgate_weight,
    decay_down, decay_up, decay_bias, head_gain, out_weight, norm_gain,
):
    vmem = pl.BlockSpec(memory_space=pltpu.VMEM)
    dma = pltpu.SemaphoreType.DMA
    return pl.pallas_call(
        functools.partial(kernel, stop),
        out_shape=jax.ShapeDtypeStruct((ROWS, D), BF16),
        in_specs=[vmem] * 14,
        out_specs=vmem,
        scratch_shapes=[
            pltpu.VMEM((3, 4, 4, 4, HID, 128), BF16),
            pltpu.VMEM((4, 4, PROJ, 128), BF16),
            pltpu.VMEM((4, 4, 4, 128, 128), BF16),
            pltpu.VMEM((PROJ + GR, D), BF16),
            pltpu.VMEM((2, ROWS, D), BF16),
            pltpu.VMEM((2, ROWS, D), BF16),
            pltpu.VMEM((768, 256), F32),
            pltpu.VMEM((256, 768), BF16),
            pltpu.VMEM((2, ROWS, D), F32),
            pltpu.VMEM((3, ROWS, D), F32),
            pltpu.VMEM((8, ROWS, D), BF16),
            pltpu.VMEM((1024, 512), F32),
            pltpu.VMEM((1024, DV), BF16),
            pltpu.VMEM((4, 256, DV), BF16),
            dma((5,)),
            dma((2, 3, 3, 2, 2)),
            dma((2, 3, 3, 2, 2)),
            dma((2, 2, 2)),
            dma((2, 2, 2)),
            dma((3, 2, 2)),
            dma((3, 2, 2)),
            dma((9,)),
            dma((9,)),
            dma((7,)),
            dma((7,)),
        ],
        compiler_params=pltpu.CompilerParams(
            collective_id=0, has_side_effects=True, vmem_limit_bytes=60 * 1024 * 1024
        ),
    )(
        stream, gate_weight.T, up_weight.T, down_weight, query_weight.T, key_weight.T, value_weight, outgate_weight,
        decay_down.T, decay_up, decay_bias[None], head_gain[None], out_weight, norm_gain,
    )


def solution(mesh, stop=0):
    in_specs = (
        P(("rep", "fs", "tp"), None),
        P("fs", "tp"),
        P("fs", "tp"),
        P("tp", "fs"),
        P("fs", "tp"),
        P("fs", "tp"),
        P("fs", "tp"),
        P("fs", "tp"),
        P(),
        P(None, "tp"),
        P("tp"),
        P(),
        P("tp", "fs"),
        P(),
    )
    return jax.shard_map(
        functools.partial(on_device, stop),
        mesh=mesh,
        in_specs=in_specs,
        out_specs=P(("rep", "fs", "tp"), None),
        check_vma=False,
    )
```

```python
import functools

import jax
import jax.numpy as jnp
from jax import lax
from jax.experimental import pallas as pl
from jax.experimental.pallas import tpu as pltpu
from jax.sharding import PartitionSpec as P

MESH = pl.DeviceIdType.MESH
F32, BF16 = jnp.float32, jnp.bfloat16
D, DK, DV, GR = 2048, 64, 128, 32
ROWS = 128
HID = 352
CHUNKS = ((0, 32, 64), (64, 160, 256), (256, 304, 352))
SECOND = ((0, HID),)
PROJ = 384
BLK = 128
RESIDUAL_SCALE = 2.0**0.5
BRANCH_SCALE = 0.5
NORM_EPS = 1e-05
HEAD_EPS = 0.01
GATE_DIVISOR = 16.0

NT = (((1,), (1,)), ((), ()))
NN = (((1,), (0,)), ((), ()))
TN = (((0,), (0,)), ((), ()))


def dot(a, b, dims=NN, **kw):
    return lax.dot_general(a, b, dims, preferred_element_type=F32, **kw)


def place():
    r, f, t = lax.axis_index("rep"), lax.axis_index("fs"), lax.axis_index("tp")
    return r, f // 4, f % 4, t // 2, t % 2


def neighbour(dim, step):
    r, zl, x, y, c = place()
    if dim == "x":
        return (r, zl * 4 + (x + step + 4) % 4, y * 2 + c)
    if dim == "y":
        return (r, zl * 4 + x, ((y + step + 4) % 4) * 2 + c)
    if dim == "c":
        return (r, zl * 4 + x, y * 2 + 1 - c)
    z = (r * 4 + zl + step + 8) % 8
    return (z // 4, (z % 4) * 4 + x, y * 2 + c)


class Gather:
    def __init__(self, order, at, rows, send, recv, pending):
        self.order, self.at, self.rows = order, at, rows
        self.send, self.recv, self.pending = send, recv, pending
        r, zl, x, y, c = place()
        self.pos = {"x": x, "y": y, "z": zl}

    def region(self, phase, shift, half):
        lo, mid, hi = self.rows
        lo, hi = ((lo, mid), (mid, hi))[half]
        idx = {}
        for k, dim in enumerate(self.order):
            if k < phase:
                idx[dim] = slice(None)
            elif k == phase:
                idx[dim] = (self.pos[dim] + shift) % 4
            else:
                idx[dim] = self.pos[dim]
        return self.at(idx, pl.ds(lo, hi - lo))

    def copy(self, phase, shift, half, stage, way):
        region = self.region(phase, shift, half)
        return pltpu.make_async_remote_copy(
            src_ref=region,
            dst_ref=region,
            send_sem=self.send(phase, stage, way),
            recv_sem=self.recv(phase, stage, way),
            device_id=neighbour(self.order[phase], 1 if way == 0 else -1),
            device_id_type=MESH,
        )

    def go(self, *args):
        cp = self.copy(*args)
        cp.start()
        self.pending.append(cp)

    def begin(self, phase):
        for stage in (0, 1):
            for way in (0, 1):
                self.go(phase, 0, way ^ stage, stage, way)

    def pass_on(self, phase):
        for way in (0, 1):
            self.copy(phase, 3 - 2 * way, way, 0, way).wait_recv()
        for way in (0, 1):
            self.go(phase, 3 - 2 * way, way, 2, way)

    def finish(self, phase):
        for way in (0, 1):
            self.copy(phase, 3 - 2 * way, 1 - way, 1, way).wait_recv()
        for way in (0, 1):
            self.copy(phase, 2, way, 2, way).wait_recv()


def layer_norm(values, norm_scale):
    average = jnp.mean(values, -1, keepdims=True)
    centred = values - average
    spread = jnp.mean(centred * centred, -1, keepdims=True)
    return (centred * lax.rsqrt(spread + NORM_EPS) * norm_scale).astype(BF16)


scope = jax.named_scope


def silu(v):
    return v / (1.0 + jnp.exp(-v))


def kernel(
    stop,
    x_ref, g_ref, u_ref, d_ref, q_ref, k_ref, v_ref, og_ref, dd_ref, du_ref, bias_ref, gain_ref, wo_ref, norm_ref,
    out_ref,
    W, Wa, Wo, WaW, xa, xb, xs, hidT, hid, acc, part, fa, proj, inner, qe, upd, shrink, level, gout, gin,
    lsem, fsend, frecv, asend, arecv, osend, orecv, csend, crecv, ysend, yrecv, hsend, hrecv,
):
    r, zl, x, y, c = place()
    t = y * 2 + c
    barrier = pltpu.get_barrier_semaphore()
    for dim in "xyz":
        for step in (1, -1):
            pl.semaphore_signal(barrier, 1, device_id=neighbour(dim, step), device_id_type=MESH)
    pl.semaphore_signal(barrier, 1, device_id=neighbour("c", 1), device_id_type=MESH)
    pl.semaphore_signal(barrier, 1, device_id=neighbour("y", 2), device_id_type=MESH)
    own = []
    for w, ref in enumerate((g_ref, u_ref, d_ref)):
        own.append(pltpu.make_async_copy(ref, W.at[w, y, zl, x], lsem.at[w]))
    own.append(pltpu.make_async_copy(wo_ref, Wo.at[y, zl, x], lsem.at[3]))
    for cp in own:
        cp.start()
    with scope("barrier"):
        pl.semaphore_wait(barrier, 8)
        for cp in own:
            cp.wait()

    pending = []

    def go(cp):
        cp.start()
        pending.append(cp)

    def settle():
        for cp in pending:
            cp.wait_send()
        pending.clear()

    def across(src, dst, slot):
        return pltpu.make_async_remote_copy(
            src_ref=src, dst_ref=dst, send_sem=csend.at[slot], recv_sem=crecv.at[slot],
            device_id=neighbour("c", 1), device_id_type=MESH,
        )

    orders = (("x", "z", "y"), ("z", "y", "x"), ("y", "x", "z"))

    def ffn_gather(ch, w):
        return Gather(
            orders[w],
            lambda idx, rows: W.at[w, idx["y"], idx["z"], idx["x"], rows],
            CHUNKS[ch],
            lambda ph, st, way: fsend.at[ch, w, ph, st, way],
            lambda ph, st, way: frecv.at[ch, w, ph, st, way],
            pending,
        )

    ffn = [[ffn_gather(ch, w) for w in range(3)] for ch in range(3)]
    ga = Gather(
        ("x", "z"), lambda idx, rows: Wa.at[idx["z"], idx["x"], rows], (0, 192, 384),
        lambda ph, st, way: asend.at[ph, st, way], lambda ph, st, way: arecv.at[ph, st, way], pending,
    )
    gw = Gather(
        ("y", "x", "z"), lambda idx, rows: Wo.at[idx["y"], idx["z"], idx["x"], rows], (0, 64, 128),
        lambda ph, st, way: osend.at[ph, st, way], lambda ph, st, way: orecv.at[ph, st, way], pending,
    )

    def begin(ch, ph):
        with scope(f"begin{ch}_{ph}"):
            for w in range(3):
                if ph:
                    ffn[ch][w].finish(ph - 1)
                ffn[ch][w].begin(ph)

    def pass_on(ch, ph):
        with scope(f"pass{ch}_{ph}"):
            for w in range(3):
                ffn[ch][w].pass_on(ph)

    def hidden(lo, hi, rows):
        size = hi - lo

        def body(yy, _):
            gate, up = (
                dot(
                    jnp.concatenate([W[w, yy, f // 4, f % 4, lo:hi, :] for f in range(16)], axis=1),
                    jnp.concatenate([rows[0], rows[1]], axis=1),
                )
                for w in (0, 1)
            )
            hidT[pl.ds(pl.multiple_of(yy * size, 16), size), :] = silu(gate) * up
            return 0

        lax.fori_loop(0, 4, body, 0, unroll=2)
        hid[:, : 4 * size] = hidT[: 4 * size, :].T.astype(BF16)

    def down(lo, hi, slot):
        size = hi - lo

        def body(j, _):
            weights = jnp.concatenate(
                [
                    jnp.concatenate([W[2, yy, j // 2, (j % 2) * 2 + i, lo:hi, :] for i in range(2)], axis=1)
                    for yy in range(4)
                ],
                axis=0,
            )
            cols = pl.ds(pl.multiple_of(j * 256, 256), 256)
            term = dot(hid[:, : 4 * size], weights)
            for half in range(2):
                piece = term[half * ROWS : (half + 1) * ROWS]
                if lo:
                    acc[half, :, cols] += piece
                else:
                    acc[half, :, cols] = piece
            return 0

        if hi == HID:
            halves(body, slot)
        else:
            lax.fori_loop(0, 8, body, 0, unroll=2)

    def give(slot, half):
        cols = pl.ds(half * 1024, 1024)
        return across(acc.at[1 - c, :, cols], part.at[slot, :, cols], 2 + 2 * slot + half)

    def halves(body, slot):
        for half in range(2):
            lax.fori_loop(half * 4, half * 4 + 4, body, 0, unroll=2)
            go(give(slot, half))

    def joined(slot, residual, scale, branch, norm):
        with scope(f"swap_{slot}"):
            for half in range(2):
                give(slot, half).wait_recv()
        with scope(f"norm_{slot}"):
            total = acc[c] + part[slot]
            return layer_norm(scale * residual.astype(F32) + branch * total, norm_ref[norm : norm + 1, :])

    for ch in range(3):
        begin(ch, 0)
    Wa[zl, x, 0:64, :] = q_ref[...]
    Wa[zl, x, 64:128, :] = k_ref[...]
    Wa[zl, x, 128:256, :] = v_ref[...].astype(F32).T.astype(BF16)
    Wa[zl, x, 256:384, :] = og_ref[...].astype(F32).T.astype(BF16)
    pass_on(0, 0)
    pass_on(1, 0)
    begin(0, 1)
    pass_on(2, 0)
    begin(1, 1)
    ga.begin(0)
    gw.begin(0)
    pass_on(0, 1)
    begin(2, 1)
    begin(0, 2)
    pass_on(1, 1)
    ga.pass_on(0)
    gw.pass_on(0)
    pass_on(2, 1)
    xa[c] = x_ref[...].astype(F32).T.astype(BF16)
    go(across(xa.at[c], xa.at[c], 0))
    pass_on(0, 2)
    begin(1, 2)
    rowi = lax.broadcasted_iota(jnp.int32, (BLK, BLK), 0)
    coli = lax.broadcasted_iota(jnp.int32, (BLK, BLK), 1)
    differ = jnp.bitwise_xor(rowi, coli)
    bits = jnp.zeros((BLK, BLK), jnp.int32)
    for k in range(7):
        bits = bits + (differ >= 2**k).astype(jnp.int32)
    level[...] = jnp.where(rowi >= coli, bits, -1)
    WaW[PROJ : PROJ + GR, :] = dd_ref[...]

    def ffn_compute(span, rows, slot):
        with scope(f"hidden{span[0]}"):
            hidden(*span, rows)
        with scope(f"down{span[0]}"):
            down(*span, slot)

    def finish(ch):
        with scope(f"finish{ch}"):
            for w in range(3):
                ffn[ch][w].finish(2)

    across(xa.at[c], xa.at[c], 0).wait_recv()
    finish(0)
    ffn_compute((0, 64), xa, 0)
    pass_on(1, 2)
    begin(2, 2)
    finish(1)
    ffn_compute((64, 256), xa, 0)
    pass_on(2, 2)
    ga.finish(0)
    ga.begin(1)
    gw.finish(0)
    gw.begin(1)
    finish(2)
    ffn_compute((256, HID), xa, 0)
    fa[t] = joined(0, x_ref[...], RESIDUAL_SCALE, BRANCH_SCALE, 0)

    half_rows = (pl.ds(0, ROWS // 2), pl.ds(ROWS // 2, ROWS // 2))

    def along(block, half, stage, way):
        ref = fa.at[block, half_rows[half]]
        return pltpu.make_async_remote_copy(
            src_ref=ref, dst_ref=ref, send_sem=ysend.at[stage, way], recv_sem=yrecv.at[stage, way],
            device_id=neighbour("y", 1 - 2 * way), device_id_type=MESH,
        )

    for stage in (0, 1):
        for way in (0, 1):
            go(along(t, way ^ stage, stage, way))

    def share(block, slot):
        return across(fa.at[block], fa.at[block], 8 + slot)

    go(share(t, 0))
    side = [((y + 3) % 4) * 2, ((y + 1) % 4) * 2]
    far = ((y + 2) % 4) * 2

    with scope("attention2"):
        ga.pass_on(1)
    with scope("attention2b"):
        gw.pass_on(1)
    with scope("rows0"):
        for way in (0, 1):
            along(side[way] + c, way, 0, way).wait_recv()
            go(along(side[way] + c, way, 2, way))
    with scope("attention3"):
        ga.finish(1)

    def widen(f, _):
        WaW[0:PROJ, pl.ds(pl.multiple_of(f * 128, 128), 128)] = Wa[f // 4, f % 4]
        return 0

    with scope("widen"):
        lax.fori_loop(0, 16, widen, 0)
    with scope("attention4"):
        gw.finish(1)
        gw.begin(2)

    def middle(b, size):
        if size >= 8:
            v = b.reshape(BLK // (2 * size), 2 * size, DK)[:, size - 1 : size, :]
            return jnp.broadcast_to(v, (BLK // (2 * size), 2 * size, DK)).reshape(BLK, DK)
        v = b.reshape(BLK // 8, 8, DK)
        sub = lax.broadcasted_iota(jnp.int32, (BLK // 8, 8, DK), 1)
        out = None
        for seg in range(8 // (2 * size)):
            at = seg * 2 * size + size - 1
            here = jnp.broadcast_to(v[:, at : at + 1, :], (BLK // 8, 8, DK))
            out = here if out is None else jnp.where(sub >= seg * 2 * size, here, out)
        return out.reshape(BLK, DK)

    def within(i):
        rows = pl.ds(pl.multiple_of(i * BLK, BLK), BLK)
        p = proj[rows, :].astype(BF16)
        q = p[:, 0:64].astype(F32) * DK**-0.5
        k = p[:, 64:128].astype(F32)
        v = p[:, 128:256]
        pre = dot(p[:, PROJ : PROJ + GR], du_ref[...]) + bias_ref[...]
        lg = (jnp.minimum(pre, 0.0) - jnp.log1p(jnp.exp(-jnp.abs(pre)))) / GATE_DIVISOR
        tri = (level[...] >= 0).astype(F32)
        b = dot(tri, lg, precision=lax.Precision.HIGHEST)
        lev = level[...]
        scores = jnp.where(lev == 0, jnp.sum(q * k, axis=1, keepdims=True), 0.0)
        for n in range(7):
            e = jnp.exp(-jnp.abs(b - middle(b, 2**n)))
            s = dot((q * e).astype(BF16), (k * e).astype(BF16), NT)
            scores = jnp.where(lev == n + 1, s, scores)
        inner[rows, :] = dot(scores.astype(BF16), v)
        qe[rows, :] = (q * jnp.exp(b)).astype(BF16)
        last = b[BLK - 1 : BLK, :]
        shrink[i] = jnp.exp(last)
        upd[i] = dot(v, (k * jnp.exp(last - b)).astype(BF16), TN)

    def project(pair):
        with scope("project"):
            rows = fa[pl.ds(pair, 2)].reshape(2 * ROWS, D)
            proj[pl.ds(pl.multiple_of(pair * ROWS, 256), 256), 0 : PROJ + GR] = dot(rows, WaW[...], NT)
        with scope("within"):
            within(pair)
            within(pair + 1)

    share(t + 1 - 2 * c, 0).wait_recv()
    project(y * 2)
    with scope("rows1"):
        for way in (0, 1):
            along(side[way] + c, 1 - way, 1, way).wait_recv()
            go(share(side[way] + c, 1 + way))
    share(side[0] + 1 - c, 1).wait_recv()
    project(side[0])
    with scope("rows2"):
        share(side[1] + 1 - c, 2).wait_recv()
    project(side[1])
    with scope("attention5"):
        gw.pass_on(2)
    with scope("rows2b"):
        for way in (0, 1):
            along(far + c, way, 2, way).wait_recv()
        go(share(far + c, 3))
    with scope("rows3"):
        share(far + 1 - c, 3).wait_recv()
    project(far)

    def home(to):
        return pltpu.make_async_remote_copy(
            src_ref=gout.at[pl.ds(to * 256, 256)], dst_ref=gin.at[y],
            send_sem=hsend.at[to], recv_sem=hrecv.at[y],
            device_id=(r, zl * 4 + x, to * 2 + c), device_id_type=MESH,
        )

    state = jnp.zeros((DV, DK), F32)
    with scope("scan"):
        for i in range(8):
            rows = pl.ds(i * BLK, BLK)
            mixed = inner[rows, :] + dot(qe[rows, :], state.astype(BF16), NT)
            state = state * shrink[i] + upd[i]
            normed = mixed * lax.rsqrt(jnp.mean(mixed * mixed, -1, keepdims=True) + HEAD_EPS) * gain_ref[...]
            gate = proj[rows, 256:384].astype(BF16).astype(F32)
            gout[rows, :] = (normed * silu(gate)).astype(BF16)
            if i % 2:

                @pl.when(y != i // 2)
                def _():
                    home(i // 2).start()

                @pl.when(y == i // 2)
                def _():
                    gin[i // 2] = gout[(i - 1) * BLK : (i + 1) * BLK, :]

    with scope("wo"):
        gw.finish(2)
    settle()
    with scope("home"):
        for step in range(1, 4):
            source = (y + step) % 4
            pltpu.make_async_remote_copy(
                src_ref=gout.at[pl.ds(0, 256)], dst_ref=gin.at[source],
                send_sem=hsend.at[source], recv_sem=hrecv.at[source],
                device_id=(r, zl * 4 + x, source * 2 + c), device_id_type=MESH,
            ).wait()

    def out_proj(j, _):
        weights = jnp.concatenate(
            [jnp.concatenate([Wo[yy, j // 2, (j % 2) * 2 + i] for i in range(2)], axis=1) for yy in range(4)],
            axis=0,
        )
        cols = pl.ds(pl.multiple_of(j * 256, 256), 256)
        term = dot(jnp.concatenate([gin[yy] for yy in range(4)], axis=1), weights)
        acc[0, :, cols] = term[:ROWS]
        acc[1, :, cols] = term[ROWS:]
        return 0

    with scope("outp"):
        halves(out_proj, 1)
    second = joined(1, fa[t], RESIDUAL_SCALE, 1.0, 1)
    xs[...] = second
    xb[c] = second.astype(F32).T.astype(BF16)
    go(across(xb.at[c], xb.at[c], 1))
    with scope("swapx"):
        across(xb.at[1 - c], xb.at[1 - c], 1).wait_recv()
    settle()
    for span in SECOND:
        ffn_compute(span, xb, 2)
    out_ref[...] = joined(2, xs[...], RESIDUAL_SCALE, BRANCH_SCALE, 2)
    if stop == 1:
        out_ref[...] = fa[t]
    if stop == 2:
        out_ref[...] = xs[...]
    settle()


def on_device(
    stop, stream, gate_weight, up_weight, down_weight, query_weight, key_weight, value_weight, outgate_weight,
    decay_down, decay_up, decay_bias, head_gain, out_weight, norm_gain,
):
    vmem = pl.BlockSpec(memory_space=pltpu.VMEM)
    dma = pltpu.SemaphoreType.DMA
    return pl.pallas_call(
        functools.partial(kernel, stop),
        out_shape=jax.ShapeDtypeStruct((ROWS, D), BF16),
        in_specs=[vmem] * 14,
        out_specs=vmem,
        scratch_shapes=[
            pltpu.VMEM((3, 4, 4, 4, HID, 128), BF16),
            pltpu.VMEM((4, 4, PROJ, 128), BF16),
            pltpu.VMEM((4, 4, 4, 128, 128), BF16),
            pltpu.VMEM((PROJ + GR, D), BF16),
            pltpu.VMEM((2, D, ROWS), BF16),
            pltpu.VMEM((2, D, ROWS), BF16),
            pltpu.VMEM((ROWS, D), BF16),
            pltpu.VMEM((4 * HID, 256), F32),
            pltpu.VMEM((256, 4 * HID), BF16),
            pltpu.VMEM((2, ROWS, D), F32),
            pltpu.VMEM((3, ROWS, D), F32),
            pltpu.VMEM((8, ROWS, D), BF16),
            pltpu.VMEM((1024, 512), F32),
            pltpu.VMEM((1024, DV), F32),
            pltpu.VMEM((1024, DK), BF16),
            pltpu.VMEM((8, DV, DK), F32),
            pltpu.VMEM((8, 1, DK), F32),
            pltpu.VMEM((BLK, BLK), jnp.int32),
            pltpu.VMEM((1024, DV), BF16),
            pltpu.VMEM((4, 256, DV), BF16),
            dma((4,)),
            dma((3, 3, 3, 3, 2)),
            dma((3, 3, 3, 3, 2)),
            dma((2, 3, 2)),
            dma((2, 3, 2)),
            dma((3, 3, 2)),
            dma((3, 3, 2)),
            dma((12,)),
            dma((12,)),
            dma((3, 2)),
            dma((3, 2)),
            dma((4,)),
            dma((4,)),
        ],
        compiler_params=pltpu.CompilerParams(
            collective_id=0, has_side_effects=True, vmem_limit_bytes=60 * 1024 * 1024
        ),
    )(
        stream, gate_weight.T, up_weight.T, down_weight, query_weight.T, key_weight.T, value_weight, outgate_weight,
        decay_down.T, decay_up, decay_bias[None], head_gain[None], out_weight, norm_gain,
    )


def solution(mesh, stop=0):
    in_specs = (
        P(("rep", "fs", "tp"), None),
        P("fs", "tp"),
        P("fs", "tp"),
        P("tp", "fs"),
        P("fs", "tp"),
        P("fs", "tp"),
        P("fs", "tp"),
        P("fs", "tp"),
        P(),
        P(None, "tp"),
        P("tp"),
        P(),
        P("tp", "fs"),
        P(),
    )
    return jax.shard_map(
        functools.partial(on_device, stop),
        mesh=mesh,
        in_specs=in_specs,
        out_specs=P(("rep", "fs", "tp"), None),
        check_vma=False,
    )
```

```python
import functools

import jax
import jax.numpy as jnp
from jax import lax
from jax.experimental import pallas as pl
from jax.experimental.pallas import tpu as pltpu
from jax.sharding import PartitionSpec as P

MESH = pl.DeviceIdType.MESH
F32, BF16 = jnp.float32, jnp.bfloat16
D, DK, DV, GR = 2048, 64, 128, 32
ROWS = 128
HID = 352
CHUNKS = ((0, 32, 64), (64, 160, 256), (256, 304, 352))
SECOND = ((0, HID),)
PROJ = 384
VMEM_LIMIT = 60 * 1024 * 1024
BLK = 128
RESIDUAL_SCALE = 2.0**0.5
BRANCH_SCALE = 0.5
NORM_EPS = 1e-05
HEAD_EPS = 0.01
GATE_DIVISOR = 16.0

NT = (((1,), (1,)), ((), ()))
NN = (((1,), (0,)), ((), ()))
TN = (((0,), (0,)), ((), ()))


def dot(a, b, dims=NN, **kw):
    return lax.dot_general(a, b, dims, preferred_element_type=F32, **kw)


def place():
    r, f, t = lax.axis_index("rep"), lax.axis_index("fs"), lax.axis_index("tp")
    return r, f // 4, f % 4, t // 2, t % 2


def neighbour(dim, step):
    r, zl, x, y, c = place()
    if dim == "x":
        return (r, zl * 4 + (x + step + 4) % 4, y * 2 + c)
    if dim == "y":
        return (r, zl * 4 + x, ((y + step + 4) % 4) * 2 + c)
    if dim == "c":
        return (r, zl * 4 + x, y * 2 + 1 - c)
    z = (r * 4 + zl + step + 8) % 8
    return (z // 4, (z % 4) * 4 + x, y * 2 + c)


class Gather:
    def __init__(self, order, at, rows, send, recv, pending):
        self.order, self.at, self.rows = order, at, rows
        self.send, self.recv, self.pending = send, recv, pending
        r, zl, x, y, c = place()
        self.pos = {"x": x, "y": y, "z": zl}

    def region(self, phase, shift, half):
        lo, mid, hi = self.rows
        lo, hi = ((lo, mid), (mid, hi))[half]
        idx = {}
        for k, dim in enumerate(self.order):
            if k < phase:
                idx[dim] = slice(None)
            elif k == phase:
                idx[dim] = (self.pos[dim] + shift) % 4
            else:
                idx[dim] = self.pos[dim]
        return self.at(idx, pl.ds(lo, hi - lo))

    def copy(self, phase, shift, half, stage, way):
        region = self.region(phase, shift, half)
        return pltpu.make_async_remote_copy(
            src_ref=region,
            dst_ref=region,
            send_sem=self.send(phase, stage, way),
            recv_sem=self.recv(phase, stage, way),
            device_id=neighbour(self.order[phase], 1 if way == 0 else -1),
            device_id_type=MESH,
        )

    def go(self, *args):
        cp = self.copy(*args)
        cp.start()
        self.pending.append(cp)

    def begin(self, phase):
        for stage in (0, 1):
            for way in (0, 1):
                self.go(phase, 0, way ^ stage, stage, way)

    def pass_on(self, phase):
        for way in (0, 1):
            self.copy(phase, 3 - 2 * way, way, 0, way).wait_recv()
        for way in (0, 1):
            self.go(phase, 3 - 2 * way, way, 2, way)

    def finish(self, phase):
        for way in (0, 1):
            self.copy(phase, 3 - 2 * way, 1 - way, 1, way).wait_recv()
        for way in (0, 1):
            self.copy(phase, 2, way, 2, way).wait_recv()


def layer_norm(values, norm_scale):
    average = jnp.mean(values, -1, keepdims=True)
    centred = values - average
    spread = jnp.mean(centred * centred, -1, keepdims=True)
    return (centred * lax.rsqrt(spread + NORM_EPS) * norm_scale).astype(BF16)


scope = jax.named_scope


def silu(v):
    return v / (1.0 + jnp.exp(-v))


def kernel(
    stop,
    x_ref, g_ref, u_ref, d_ref, q_ref, k_ref, v_ref, og_ref, dd_ref, du_ref, bias_ref, gain_ref, wo_ref, norm_ref,
    out_ref,
    W, Wa, Wo, WaW, xa, xb, xs, hidT, hid, acc, part, fa, proj, inner, qe, upd, shrink, gate, du2, bias2, level,
    gout, gin,
    lsem, fsend, frecv, asend, arecv, osend, orecv, csend, crecv, ysend, yrecv, hsend, hrecv,
):
    r, zl, x, y, c = place()
    t = y * 2 + c
    barrier = pltpu.get_barrier_semaphore()
    for dim in "xyz":
        for step in (1, -1):
            pl.semaphore_signal(barrier, 1, device_id=neighbour(dim, step), device_id_type=MESH)
    pl.semaphore_signal(barrier, 1, device_id=neighbour("c", 1), device_id_type=MESH)
    pl.semaphore_signal(barrier, 1, device_id=neighbour("y", 2), device_id_type=MESH)
    own = []
    for w, ref in enumerate((g_ref, u_ref, d_ref)):
        own.append(pltpu.make_async_copy(ref, W.at[w, y, zl, x], lsem.at[w]))
    own.append(pltpu.make_async_copy(wo_ref, Wo.at[y, zl, x], lsem.at[3]))
    for cp in own:
        cp.start()
    with scope("barrier"):
        pl.semaphore_wait(barrier, 8)
        for cp in own:
            cp.wait()

    pending = []

    def go(cp):
        cp.start()
        pending.append(cp)

    def settle():
        for cp in pending:
            cp.wait_send()
        pending.clear()

    def across(src, dst, slot):
        return pltpu.make_async_remote_copy(
            src_ref=src, dst_ref=dst, send_sem=csend.at[slot], recv_sem=crecv.at[slot],
            device_id=neighbour("c", 1), device_id_type=MESH,
        )

    orders = (("x", "z", "y"), ("z", "y", "x"), ("y", "x", "z"))

    def ffn_gather(ch, w):
        return Gather(
            orders[w],
            lambda idx, rows: W.at[w, idx["y"], idx["z"], idx["x"], rows],
            CHUNKS[ch],
            lambda ph, st, way: fsend.at[ch, w, ph, st, way],
            lambda ph, st, way: frecv.at[ch, w, ph, st, way],
            pending,
        )

    ffn = [[ffn_gather(ch, w) for w in range(3)] for ch in range(3)]
    ga = [
        Gather(
            order, lambda idx, rows: Wa.at[idx["z"], idx["x"], rows], span,
            lambda ph, st, way, n=n: asend.at[n, ph, st, way], lambda ph, st, way, n=n: arecv.at[n, ph, st, way],
            pending,
        )
        for n, (order, span) in enumerate(((("x", "z"), (0, 96, 192)), (("z", "x"), (192, 288, 384))))
    ]
    gw = [
        Gather(
            order, lambda idx, rows: Wo.at[idx["y"], idx["z"], idx["x"], rows], span,
            lambda ph, st, way, n=n: osend.at[n, ph, st, way], lambda ph, st, way, n=n: orecv.at[n, ph, st, way],
            pending,
        )
        for n, (order, span) in enumerate(((("y", "x", "z"), (0, 32, 64)), (("y", "z", "x"), (64, 96, 128))))
    ]

    def each(gathers, op, phase):
        for g in gathers:
            getattr(g, op)(phase)

    def begin(ch, ph):
        with scope(f"begin{ch}_{ph}"):
            for w in range(3):
                if ph:
                    ffn[ch][w].finish(ph - 1)
                ffn[ch][w].begin(ph)

    def pass_on(ch, ph):
        with scope(f"pass{ch}_{ph}"):
            for w in range(3):
                ffn[ch][w].pass_on(ph)

    def hidden(lo, hi, rows):
        size = hi - lo

        def body(yy, _):
            gate, up = (
                dot(
                    jnp.concatenate([W[w, yy, f // 4, f % 4, lo:hi, :] for f in range(16)], axis=1),
                    jnp.concatenate([rows[0], rows[1]], axis=1),
                )
                for w in (0, 1)
            )
            hidT[pl.ds(pl.multiple_of(yy * size, 16), size), :] = silu(gate) * up
            return 0

        lax.fori_loop(0, 4, body, 0, unroll=True)
        hid[:, : 4 * size] = hidT[: 4 * size, :].T.astype(BF16)

    def down(lo, hi, slot):
        size = hi - lo

        def body(j, _):
            weights = jnp.concatenate(
                [
                    jnp.concatenate([W[2, yy, j // 2, (j % 2) * 2 + i, lo:hi, :] for i in range(2)], axis=1)
                    for yy in range(4)
                ],
                axis=0,
            )
            cols = pl.ds(pl.multiple_of(j * 256, 256), 256)
            term = dot(hid[:, : 4 * size], weights)
            for half in range(2):
                piece = term[half * ROWS : (half + 1) * ROWS]
                if lo:
                    acc[half, :, cols] += piece
                else:
                    acc[half, :, cols] = piece
            return 0

        if hi == HID:
            pieces(body, slot)
        else:
            lax.fori_loop(0, 8, body, 0, unroll=2)

    def give(slot, piece):
        cols = pl.ds(piece * 512, 512)
        return across(acc.at[1 - c, :, cols], part.at[slot, :, cols], 2 + 4 * slot + piece)

    def pieces(body, slot):
        for piece in range(4):
            lax.fori_loop(piece * 2, piece * 2 + 2, body, 0, unroll=True)
            go(give(slot, piece))

    def joined(slot, residual, scale, branch, norm):
        with scope(f"swap_{slot}"):
            for piece in range(4):
                give(slot, piece).wait_recv()
        with scope(f"norm_{slot}"):
            total = acc[c] + part[slot]
            return layer_norm(scale * residual.astype(F32) + branch * total, norm_ref[norm : norm + 1, :])

    for ch in range(3):
        begin(ch, 0)
    Wa[zl, x, 0:64, :] = q_ref[...]
    Wa[zl, x, 64:128, :] = k_ref[...]
    Wa[zl, x, 128:256, :] = v_ref[...].astype(F32).T.astype(BF16)
    Wa[zl, x, 256:384, :] = og_ref[...].astype(F32).T.astype(BF16)
    pass_on(0, 0)
    pass_on(1, 0)
    begin(0, 1)
    pass_on(2, 0)
    begin(1, 1)
    each(ga, "begin", 0)
    each(gw, "begin", 0)
    pass_on(0, 1)
    begin(2, 1)
    begin(0, 2)
    pass_on(1, 1)
    each(ga, "pass_on", 0)
    each(gw, "pass_on", 0)
    pass_on(2, 1)
    xa[c] = x_ref[...].astype(F32).T.astype(BF16)
    go(across(xa.at[c], xa.at[c], 0))
    pass_on(0, 2)
    begin(1, 2)
    for half in range(2):
        du2[:, half * DK : (half + 1) * DK] = du_ref[...]
        bias2[:, half * DK : (half + 1) * DK] = bias_ref[...]
    rowi = lax.broadcasted_iota(jnp.int32, (BLK, BLK), 0)
    coli = lax.broadcasted_iota(jnp.int32, (BLK, BLK), 1)
    differ = jnp.bitwise_xor(rowi, coli)
    bits = jnp.zeros((BLK, BLK), jnp.int32)
    for k in range(7):
        bits = bits + (differ >= 2**k).astype(jnp.int32)
    level[...] = jnp.where(rowi >= coli, bits, -1)
    WaW[PROJ : PROJ + GR, :] = dd_ref[...]

    def ffn_compute(span, rows, slot):
        with scope(f"hidden{span[0]}"):
            hidden(*span, rows)
        with scope(f"down{span[0]}"):
            down(*span, slot)

    def finish(ch):
        with scope(f"finish{ch}"):
            for w in range(3):
                ffn[ch][w].finish(2)

    across(xa.at[c], xa.at[c], 0).wait_recv()
    finish(0)
    ffn_compute((0, 64), xa, 0)
    pass_on(1, 2)
    begin(2, 2)
    finish(1)
    ffn_compute((64, 256), xa, 0)
    pass_on(2, 2)
    each(ga, "finish", 0)
    each(ga, "begin", 1)
    each(gw, "finish", 0)
    each(gw, "begin", 1)
    finish(2)
    ffn_compute((256, HID), xa, 0)
    fa[t] = joined(0, x_ref[...], RESIDUAL_SCALE, BRANCH_SCALE, 0)

    half_rows = (pl.ds(0, ROWS // 2), pl.ds(ROWS // 2, ROWS // 2))

    def along(block, half, stage, way):
        ref = fa.at[block, half_rows[half]]
        return pltpu.make_async_remote_copy(
            src_ref=ref, dst_ref=ref, send_sem=ysend.at[stage, way], recv_sem=yrecv.at[stage, way],
            device_id=neighbour("y", 1 - 2 * way), device_id_type=MESH,
        )

    for stage in (0, 1):
        for way in (0, 1):
            go(along(t, way ^ stage, stage, way))

    def share(block, half, slot):
        ref = fa.at[block, half_rows[half]]
        return across(ref, ref, 14 + 2 * slot + half)

    go(share(t, 0, 0))
    go(share(t, 1, 0))
    side = [((y + 3) % 4) * 2, ((y + 1) % 4) * 2]
    far = ((y + 2) % 4) * 2

    with scope("attention2"):
        each(ga, "pass_on", 1)
    with scope("attention2b"):
        each(gw, "pass_on", 1)
    with scope("rows0"):
        for way in (0, 1):
            along(side[way] + c, way, 0, way).wait_recv()
            go(along(side[way] + c, way, 2, way))
            go(share(side[way] + c, way, 1 + way))
    with scope("attention3"):
        each(ga, "finish", 1)
    with scope("attention4"):
        each(gw, "finish", 1)
        each(gw, "begin", 2)

    def widen(f, _):
        WaW[0:PROJ, pl.ds(pl.multiple_of(f * 128, 128), 128)] = Wa[f // 4, f % 4]
        return 0

    with scope("widen"):
        lax.fori_loop(0, 16, widen, 0)

    def middle(b, size):
        if size >= 8:
            v = b.reshape(BLK // (2 * size), 2 * size, 2 * DK)[:, size - 1 : size, :]
            return jnp.broadcast_to(v, (BLK // (2 * size), 2 * size, 2 * DK)).reshape(BLK, 2 * DK)
        v = b.reshape(BLK // 8, 8, 2 * DK)
        sub = lax.broadcasted_iota(jnp.int32, (BLK // 8, 8, 2 * DK), 1)
        out = None
        for seg in range(8 // (2 * size)):
            at = seg * 2 * size + size - 1
            here = jnp.broadcast_to(v[:, at : at + 1, :], (BLK // 8, 8, 2 * DK))
            out = here if out is None else jnp.where(sub >= seg * 2 * size, here, out)
        return out.reshape(BLK, 2 * DK)

    def within(pair):
        spans = [pl.ds(pl.multiple_of((pair + n) * BLK, BLK), BLK) for n in range(2)]
        p = [proj[rows, :] for rows in spans]
        qk = [one[:, 0 : 2 * DK].astype(F32) for one in p]
        left = lax.broadcasted_iota(jnp.int32, (BLK, 2 * DK), 1) < DK
        q = jnp.where(left, qk[0], pltpu.roll(qk[1], DK, 1)) * DK**-0.5
        k = jnp.where(left, pltpu.roll(qk[0], DK, 1), qk[1])
        pre = [dot(one[:, PROJ : PROJ + GR], du2[...]) for one in p]
        pre = jnp.where(left, pre[0], pre[1]) + bias2[...]
        lg = (jnp.minimum(pre, 0.0) - jnp.log1p(jnp.exp(-jnp.abs(pre)))) / GATE_DIVISOR
        lev = level[...]
        tri = (lev >= 0).astype(BF16)
        b = jnp.zeros((BLK, 2 * DK), F32)
        for _ in range(3):
            top = lg.astype(BF16)
            b = b + dot(tri, top)
            lg = lg - top.astype(F32)

        def halves_of(values):
            values = values.astype(BF16)
            zero = jnp.zeros_like(values)
            return [jnp.where(left, values, zero), jnp.where(left, zero, values)]

        scores = None
        for n in range(8):
            if n:
                e = jnp.exp(-jnp.abs(b - middle(b, 2 ** (n - 1))))
                s = dot(jnp.concatenate(halves_of(q * e), axis=0), (k * e).astype(BF16), NT)
                scores = [jnp.where(lev == n, s[m * BLK : (m + 1) * BLK], scores[m]) for m in range(2)]
            else:
                s = dot(jnp.concatenate(halves_of(q), axis=0), k.astype(BF16), NT)
                scores = [jnp.where(lev == 0, s[m * BLK : (m + 1) * BLK], 0.0) for m in range(2)]
        last = b[BLK - 1 : BLK, :]
        carry = (k * jnp.exp(last - b)).astype(BF16)
        ends = halves_of(q * jnp.exp(b))
        fade = jnp.exp(jnp.broadcast_to(last, (8, 2 * DK)))
        for m in range(2):
            v = p[m][:, 128:256]
            inner[spans[m], :] = dot(scores[m].astype(BF16), v)
            qe[pair + m] = ends[m]
            both = [dot(v, carry, TN), fade]
            both = [
                jnp.where(lax.broadcasted_iota(jnp.int32, one.shape, 1) < DK, *((one, pltpu.roll(one, DK, 1))[:: 1 - 2 * m]))
                for one in both
            ]
            upd[pair + m] = both[0]
            shrink[pair + m] = both[1]
            gate[spans[m], :] = silu(p[m][:, 256:384].astype(F32)) * gain_ref[...]

    def arrived(block, slot):
        for half in range(2):
            share(block, half, slot).wait_recv()

    def project(pair):
        with scope("project"):
            rows = fa[pl.ds(pair, 2)].reshape(2 * ROWS, D)
            proj[pl.ds(pl.multiple_of(pair * ROWS, 256), 256), 0 : PROJ + GR] = dot(rows, WaW[...], NT).astype(BF16)
        with scope("within"):
            within(pair)

    arrived(t + 1 - 2 * c, 0)
    project(y * 2)
    with scope("rows1"):
        for way in (0, 1):
            along(side[way] + c, 1 - way, 1, way).wait_recv()
            go(share(side[way] + c, 1 - way, 1 + way))
    with scope("rows1b"):
        arrived(side[0] + 1 - c, 1)
    project(side[0])
    with scope("rows2"):
        arrived(side[1] + 1 - c, 2)
    project(side[1])
    with scope("attention5"):
        each(gw, "pass_on", 2)
    with scope("rows2b"):
        for way in (0, 1):
            along(far + c, way, 2, way).wait_recv()
            go(share(far + c, way, 3))
    with scope("rows3"):
        arrived(far + 1 - c, 3)
    project(far)

    def home(to):
        return pltpu.make_async_remote_copy(
            src_ref=gout.at[pl.ds(to * 256, 256)], dst_ref=gin.at[y],
            send_sem=hsend.at[to], recv_sem=hrecv.at[y],
            device_id=(r, zl * 4 + x, to * 2 + c), device_id_type=MESH,
        )

    state = jnp.zeros((DV, 2 * DK), F32)
    with scope("scan"):
        for i in range(8):
            rows = pl.ds(i * BLK, BLK)
            mixed = inner[rows, :] + dot(qe[i], state.astype(BF16), NT)
            state = state * shrink[i, 0:1] + upd[i]
            spread = jnp.mean(mixed * mixed, -1, keepdims=True)
            gout[rows, :] = (mixed * lax.rsqrt(spread + HEAD_EPS) * gate[rows, :]).astype(BF16)
            if i % 2:

                @pl.when(y != i // 2)
                def _():
                    home(i // 2).start()

                @pl.when(y == i // 2)
                def _():
                    gin[i // 2] = gout[(i - 1) * BLK : (i + 1) * BLK, :]

    with scope("wo"):
        each(gw, "finish", 2)
    settle()
    with scope("home"):
        for step in range(1, 4):
            source = (y + step) % 4
            pltpu.make_async_remote_copy(
                src_ref=gout.at[pl.ds(0, 256)], dst_ref=gin.at[source],
                send_sem=hsend.at[source], recv_sem=hrecv.at[source],
                device_id=(r, zl * 4 + x, source * 2 + c), device_id_type=MESH,
            ).wait()

    def out_proj(j, _):
        weights = jnp.concatenate(
            [jnp.concatenate([Wo[yy, j // 2, (j % 2) * 2 + i] for i in range(2)], axis=1) for yy in range(4)],
            axis=0,
        )
        cols = pl.ds(pl.multiple_of(j * 256, 256), 256)
        term = dot(jnp.concatenate([gin[yy] for yy in range(4)], axis=1), weights)
        acc[0, :, cols] = term[:ROWS]
        acc[1, :, cols] = term[ROWS:]
        return 0

    with scope("outp"):
        pieces(out_proj, 1)
    second = joined(1, fa[t], RESIDUAL_SCALE, 1.0, 1)
    xs[...] = second
    xb[c] = second.astype(F32).T.astype(BF16)
    go(across(xb.at[c], xb.at[c], 1))
    with scope("swapx"):
        across(xb.at[1 - c], xb.at[1 - c], 1).wait_recv()
    settle()
    for span in SECOND:
        ffn_compute(span, xb, 2)
    out_ref[...] = joined(2, xs[...], RESIDUAL_SCALE, BRANCH_SCALE, 2)
    if stop == 1:
        out_ref[...] = fa[t]
    if stop == 2:
        out_ref[...] = xs[...]
    settle()


def on_device(
    stop, stream, gate_weight, up_weight, down_weight, query_weight, key_weight, value_weight, outgate_weight,
    decay_down, decay_up, decay_bias, head_gain, out_weight, norm_gain,
):
    vmem = pl.BlockSpec(memory_space=pltpu.VMEM)
    dma = pltpu.SemaphoreType.DMA
    return pl.pallas_call(
        functools.partial(kernel, stop),
        out_shape=jax.ShapeDtypeStruct((ROWS, D), BF16),
        in_specs=[vmem] * 14,
        out_specs=vmem,
        scratch_shapes=[
            pltpu.VMEM((3, 4, 4, 4, HID, 128), BF16),
            pltpu.VMEM((4, 4, PROJ, 128), BF16),
            pltpu.VMEM((4, 4, 4, 128, 128), BF16),
            pltpu.VMEM((PROJ + GR, D), BF16),
            pltpu.VMEM((2, D, ROWS), BF16),
            pltpu.VMEM((2, D, ROWS), BF16),
            pltpu.VMEM((ROWS, D), BF16),
            pltpu.VMEM((4 * HID, 256), F32),
            pltpu.VMEM((256, 4 * HID), BF16),
            pltpu.VMEM((2, ROWS, D), F32),
            pltpu.VMEM((3, ROWS, D), F32),
            pltpu.VMEM((8, ROWS, D), BF16),
            pltpu.VMEM((1024, 512), BF16),
            pltpu.VMEM((1024, DV), F32),
            pltpu.VMEM((8, BLK, 2 * DK), BF16),
            pltpu.VMEM((8, DV, 2 * DK), F32),
            pltpu.VMEM((8, 8, 2 * DK), F32),
            pltpu.VMEM((1024, DV), F32),
            pltpu.VMEM((GR, 2 * DK), BF16),
            pltpu.VMEM((1, 2 * DK), F32),
            pltpu.VMEM((BLK, BLK), jnp.int32),
            pltpu.VMEM((1024, DV), BF16),
            pltpu.VMEM((4, 256, DV), BF16),
            dma((4,)),
            dma((3, 3, 3, 3, 2)),
            dma((3, 3, 3, 3, 2)),
            dma((2, 2, 3, 2)),
            dma((2, 2, 3, 2)),
            dma((2, 3, 3, 2)),
            dma((2, 3, 3, 2)),
            dma((22,)),
            dma((22,)),
            dma((3, 2)),
            dma((3, 2)),
            dma((4,)),
            dma((4,)),
        ],
        compiler_params=pltpu.CompilerParams(
            collective_id=0, has_side_effects=True, vmem_limit_bytes=VMEM_LIMIT
        ),
    )(
        stream, gate_weight.T, up_weight.T, down_weight, query_weight.T, key_weight.T, value_weight, outgate_weight,
        decay_down.T, decay_up, decay_bias[None], head_gain[None], out_weight, norm_gain,
    )


def solution(mesh, stop=0):
    in_specs = (
        P(("rep", "fs", "tp"), None),
        P("fs", "tp"),
        P("fs", "tp"),
        P("tp", "fs"),
        P("fs", "tp"),
        P("fs", "tp"),
        P("fs", "tp"),
        P("fs", "tp"),
        P(),
        P(None, "tp"),
        P("tp"),
        P(),
        P("tp", "fs"),
        P(),
    )
    return jax.shard_map(
        functools.partial(on_device, stop),
        mesh=mesh,
        in_specs=in_specs,
        out_specs=P(("rep", "fs", "tp"), None),
        check_vma=False,
    )
```

```python
import functools

import jax
import jax.numpy as jnp
from jax import lax
from jax.experimental import pallas as pl
from jax.experimental.pallas import tpu as pltpu
from jax.sharding import PartitionSpec as P

MESH = pl.DeviceIdType.MESH
F32, BF16 = jnp.float32, jnp.bfloat16
D, DK, DV, GR = 2048, 64, 128, 32
ROWS = 128
HID = 352
CHUNKS = ((0, 32, 64), (64, 160, 256), (256, 304, 352))
SECOND = ((0, HID),)
PROJ = 384
DIRECT = True
VMEM_LIMIT = 60 * 1024 * 1024
BLK = 128
RESIDUAL_SCALE = 2.0**0.5
BRANCH_SCALE = 0.5
NORM_EPS = 1e-05
HEAD_EPS = 0.01
GATE_DIVISOR = 16.0

NT = (((1,), (1,)), ((), ()))
NN = (((1,), (0,)), ((), ()))
TN = (((0,), (0,)), ((), ()))


def dot(a, b, dims=NN, **kw):
    return lax.dot_general(a, b, dims, preferred_element_type=F32, **kw)


def place():
    r, f, t = lax.axis_index("rep"), lax.axis_index("fs"), lax.axis_index("tp")
    return r, f // 4, f % 4, t // 2, t % 2


def neighbour(dim, step):
    r, zl, x, y, c = place()
    if dim == "x":
        return (r, zl * 4 + (x + step + 4) % 4, y * 2 + c)
    if dim == "y":
        return (r, zl * 4 + x, ((y + step + 4) % 4) * 2 + c)
    if dim == "c":
        return (r, zl * 4 + x, y * 2 + 1 - c)
    z = (r * 4 + zl + step + 8) % 8
    return (z // 4, (z % 4) * 4 + x, y * 2 + c)


class Gather:
    def __init__(self, order, at, rows, send, recv, direct=()):
        self.order, self.at, self.rows = order, at, rows
        self.send, self.recv, self.direct = send, recv, direct
        r, zl, x, y, c = place()
        self.pos = {"x": x, "y": y, "z": zl}

    def region(self, phase, along, lo, hi):
        idx = {}
        for k, dim in enumerate(self.order):
            if k < phase:
                idx[dim] = slice(None)
            elif k == phase:
                idx[dim] = along
            else:
                idx[dim] = self.pos[dim]
        return self.at(idx, pl.ds(lo, hi - lo))

    def copy(self, phase, region, late, step):
        return pltpu.make_async_remote_copy(
            src_ref=region,
            dst_ref=region,
            send_sem=self.send(phase),
            recv_sem=self.recv(phase, late),
            device_id=neighbour(self.order[phase], step),
            device_id_type=MESH,
        )

    def go(self, phase, shift, half, late, step):
        lo, mid, hi = self.rows
        lo, hi = ((lo, mid), (mid, hi))[half]
        self.copy(phase, self.region(phase, (self.pos[self.order[phase]] + shift) % 4, lo, hi), late, step).start()

    def whole(self, phase, count, late, lo, hi):
        return self.copy(phase, self.region(phase, pl.ds(0, count), lo, hi), late, 1)

    def begin(self, phase):
        for late in (0, 1):
            for way in (0, 1):
                self.go(phase, 0, way ^ late, late, 1 - 2 * way)
        if phase in self.direct:
            for way in (0, 1):
                self.go(phase, 0, way, 1, 2 - 4 * way)

    def first_halves(self, phase):
        self.whole(phase, 1, 0, self.rows[0], self.rows[2]).wait_recv()

    def pass_on(self, phase):
        if phase not in self.direct:
            self.first_halves(phase)
            for way in (0, 1):
                self.go(phase, 3 - 2 * way, way, 1, 1 - 2 * way)

    def finish(self, phase):
        if phase in self.direct:
            self.first_halves(phase)
        self.whole(phase, 2, 1, self.rows[0], self.rows[2]).wait_recv()

    def sent(self, phase, lo, hi):
        self.whole(phase, 3, 0, lo, hi).wait_send()


def layer_norm(values, norm_scale):
    average = jnp.mean(values, -1, keepdims=True)
    centred = values - average
    spread = jnp.mean(centred * centred, -1, keepdims=True)
    return (centred * lax.rsqrt(spread + NORM_EPS) * norm_scale).astype(BF16)


scope = jax.named_scope


def column_block(j):
    return pl.ds(j * 256 if isinstance(j, int) else pl.multiple_of(j * 256, 256), 256)


def silu(v):
    return v / (1.0 + jnp.exp(-v))


def kernel(
    stop,
    x_hbm, g_ref, u_ref, d_ref, q_hbm, k_hbm, v_hbm, og_hbm, dd_hbm, du_ref, bias_ref, gain_ref, wo_ref, norm_ref,
    out_ref,
    x_ref, q_ref, k_ref, v_ref, og_ref, W, Wa, Wo, WaW, xa, xb, xs, hidT, hid, acc, part, fa, proj, inner, qe, upd, shrink, gate, du2, bias2, level,
    gout, gin,
    lsem, fsend, frecv, asend, arecv, osend, orecv, csend, crecv, ysend, yrecv, hsend, hrecv,
):
    r, zl, x, y, c = place()
    t = y * 2 + c
    barrier = pltpu.get_barrier_semaphore()
    for dim in "xyz":
        for step in (1, -1, 2, -2) if dim == "z" else (1, -1, 2):
            pl.semaphore_signal(barrier, 1, device_id=neighbour(dim, step), device_id_type=MESH)
    pl.semaphore_signal(barrier, 1, device_id=neighbour("c", 1), device_id_type=MESH)
    own = []
    for w, ref in enumerate((g_ref, u_ref, d_ref)):
        own.append(pltpu.make_async_copy(ref, W.at[w, y, zl, x], lsem.at[w]))
    later = [pltpu.make_async_copy(wo_ref, Wo.at[y, zl, x], lsem.at[3])]
    for src, dst in (
        (q_hbm, q_ref),
        (k_hbm, k_ref),
        (v_hbm, v_ref),
        (og_hbm, og_ref),
        (dd_hbm, WaW.at[PROJ : PROJ + GR]),
        (x_hbm, x_ref),
    ):
        later.append(pltpu.make_async_copy(src, dst, lsem.at[3 + len(later)]))
    for cp in own + later:
        cp.start()
    with scope("barrier"):
        pl.semaphore_wait(barrier, 11)
        for cp in own:
            cp.wait()

    pending = []

    def go(cp):
        cp.start()
        pending.append(cp)

    def settle():
        for cp in pending:
            cp.wait_send()
        pending.clear()

    def across(src, dst, slot):
        return pltpu.make_async_remote_copy(
            src_ref=src, dst_ref=dst, send_sem=csend.at[slot], recv_sem=crecv.at[slot],
            device_id=neighbour("c", 1), device_id_type=MESH,
        )

    orders = (("x", "z", "y"), ("z", "y", "x"), ("y", "x", "z"))

    def ffn_gather(ch, w):
        return Gather(
            orders[w],
            lambda idx, rows: W.at[w, idx["y"], idx["z"], idx["x"], rows],
            CHUNKS[ch],
            lambda ph: fsend.at[w, ph],
            lambda ph, late: frecv.at[ch, w, ph, late],
            (0,) if ch == 0 and DIRECT else (),
        )

    ffn = [[ffn_gather(ch, w) for w in range(3)] for ch in range(3)]
    ga = [
        Gather(
            order, lambda idx, rows: Wa.at[idx["z"], idx["x"], rows], span,
            lambda ph, n=n: asend.at[n, ph], lambda ph, late, n=n: arecv.at[n, ph, late],
        )
        for n, (order, span) in enumerate(((("x", "z"), (0, 96, 192)), (("z", "x"), (192, 288, 384))))
    ]
    gw = [
        Gather(
            order, lambda idx, rows: Wo.at[idx["y"], idx["z"], idx["x"], rows], span,
            lambda ph, n=n: osend.at[n, ph], lambda ph, late, n=n: orecv.at[n, ph, late],
        )
        for n, (order, span) in enumerate(((("y", "x", "z"), (0, 32, 64)), (("y", "z", "x"), (64, 96, 128))))
    ]

    def each(gathers, op, phase):
        for g in gathers:
            getattr(g, op)(phase)

    def begin(ch, ph):
        with scope(f"begin{ch}_{ph}"):
            for w in range(3):
                if ph:
                    ffn[ch][w].finish(ph - 1)
                ffn[ch][w].begin(ph)

    def pass_on(ch, ph):
        with scope(f"pass{ch}_{ph}"):
            for w in range(3):
                ffn[ch][w].pass_on(ph)

    def hidden(lo, hi, rows):
        size = hi - lo

        def body(yy, _):
            both = [
                jnp.concatenate([W[w, yy, f // 4, f % 4, lo:hi, :] for f in range(16)], axis=1) for w in (0, 1)
            ]
            if size < 128:
                both = [jnp.concatenate(both, axis=0)]
            wide = jnp.concatenate([rows[0], rows[1]], axis=1)
            products = [dot(one, wide) for one in both]
            gate = products[0][:size]
            up = products[-1][-size:]
            hidT[pl.ds(pl.multiple_of(yy * size, 16), size), :] = silu(gate) * up
            return 0

        lax.fori_loop(0, 4, body, 0, unroll=True)
        hid[:, : 4 * size] = hidT[: 4 * size, :].T.astype(BF16)

    def down(lo, hi, slot):
        size = hi - lo

        def weights(j):
            return jnp.concatenate(
                [
                    jnp.concatenate([W[2, yy, j // 2, (j % 2) * 2 + i, lo:hi, :] for i in range(2)], axis=1)
                    for yy in range(4)
                ],
                axis=0,
            )

        def body(j, _):
            term = dot(hid[:, : 4 * size], weights(j))
            for half in range(2):
                piece = term[half * ROWS : (half + 1) * ROWS]
                if lo:
                    acc[half, :, column_block(j)] += piece
                else:
                    acc[half, :, column_block(j)] = piece
            return 0

        def one(j, who):
            term = dot(hid[rows_of(who), : 4 * size], weights(j))
            if lo:
                acc[who, :, column_block(j)] += term
            else:
                acc[who, :, column_block(j)] = term

        if hi == HID:
            pieces(one, slot)
        else:
            lax.fori_loop(0, 8, body, 0, unroll=2)

    def rows_of(who):
        return pl.ds(pl.multiple_of(who * ROWS, ROWS), ROWS)

    def give(slot, piece):
        cols = pl.ds(piece * 512, 512)
        return across(acc.at[1 - c, :, cols], part.at[slot, :, cols], 2 + slot)

    def given(slot):
        return across(acc.at[1 - c], part.at[slot], 2 + slot)

    def pieces(one, slot):
        for piece in range(4):
            for j in range(piece * 2, piece * 2 + 2):
                one(j, 1 - c)
            give(slot, piece).start()
        pending.append(given(slot))
        for j in range(8):
            one(j, c)

    def joined(slot, residual, scale, branch, norm):
        with scope(f"swap_{slot}"):
            given(slot).wait_recv()
        with scope(f"norm_{slot}"):
            total = acc[c] + part[slot]
            return layer_norm(scale * residual.astype(F32) + branch * total, norm_ref[norm : norm + 1, :])

    for ch in range(3):
        begin(ch, 0)
    for cp in later:
        cp.wait()
    Wa[zl, x, 0:64, :] = q_ref[...]
    Wa[zl, x, 64:128, :] = k_ref[...]
    Wa[zl, x, 128:256, :] = v_ref[...].astype(F32).T.astype(BF16)
    Wa[zl, x, 256:384, :] = og_ref[...].astype(F32).T.astype(BF16)
    pass_on(0, 0)
    pass_on(1, 0)
    begin(0, 1)
    pass_on(2, 0)
    begin(1, 1)
    each(ga, "begin", 0)
    each(gw, "begin", 0)
    pass_on(0, 1)
    begin(2, 1)
    begin(0, 2)
    pass_on(1, 1)
    each(ga, "pass_on", 0)
    each(gw, "pass_on", 0)
    pass_on(2, 1)
    xa[c] = x_ref[...].astype(F32).T.astype(BF16)
    go(across(xa.at[c], xa.at[c], 0))
    pass_on(0, 2)
    begin(1, 2)
    for half in range(2):
        du2[:, half * DK : (half + 1) * DK] = du_ref[...]
        bias2[:, half * DK : (half + 1) * DK] = bias_ref[...]
    rowi = lax.broadcasted_iota(jnp.int32, (BLK, BLK), 0)
    coli = lax.broadcasted_iota(jnp.int32, (BLK, BLK), 1)
    differ = jnp.bitwise_xor(rowi, coli)
    bits = jnp.zeros((BLK, BLK), jnp.int32)
    for k in range(7):
        bits = bits + (differ >= 2**k).astype(jnp.int32)
    level[...] = jnp.where(rowi >= coli, bits, -1)

    def ffn_compute(span, rows, slot):
        with scope(f"hidden{span[0]}"):
            hidden(*span, rows)
        with scope(f"down{span[0]}"):
            down(*span, slot)

    def finish(ch):
        with scope(f"finish{ch}"):
            for w in range(3):
                ffn[ch][w].finish(2)

    across(xa.at[c], xa.at[c], 0).wait_recv()
    finish(0)
    ffn_compute((0, 64), xa, 0)
    pass_on(1, 2)
    begin(2, 2)
    finish(1)
    ffn_compute((64, 256), xa, 0)
    pass_on(2, 2)
    each(ga, "finish", 0)
    each(ga, "begin", 1)
    each(gw, "finish", 0)
    each(gw, "begin", 1)
    finish(2)
    ffn_compute((256, HID), xa, 0)
    fa[t] = joined(0, x_ref[...], RESIDUAL_SCALE, BRANCH_SCALE, 0)

    half_rows = (pl.ds(0, ROWS // 2), pl.ds(ROWS // 2, ROWS // 2))

    def along(block, half, stage, way):
        ref = fa.at[block, half_rows[half]]
        return pltpu.make_async_remote_copy(
            src_ref=ref, dst_ref=ref, send_sem=ysend.at[stage, way], recv_sem=yrecv.at[stage, way],
            device_id=neighbour("y", 1 - 2 * way), device_id_type=MESH,
        )

    for stage in (0, 1):
        for way in (0, 1):
            go(along(t, way ^ stage, stage, way))

    def share(block, half, slot):
        ref = fa.at[block, half_rows[half]]
        across(ref, ref, 5 + slot).start()

    def shared(block, slot):
        return across(fa.at[block], fa.at[block], 5 + slot)

    go(shared(t, 0))
    side = [((y + 3) % 4) * 2, ((y + 1) % 4) * 2]
    far = ((y + 2) % 4) * 2

    with scope("attention2"):
        each(ga, "pass_on", 1)
    with scope("attention2b"):
        each(gw, "pass_on", 1)
    with scope("rows0"):
        for way in (0, 1):
            along(side[way] + c, way, 0, way).wait_recv()
            go(along(side[way] + c, way, 2, way))
            share(side[way] + c, way, 1 + way)
    with scope("attention3"):
        each(ga, "finish", 1)
    with scope("attention4"):
        each(gw, "finish", 1)
        each(gw, "begin", 2)

    def widen(f, _):
        WaW[0:PROJ, pl.ds(pl.multiple_of(f * 128, 128), 128)] = Wa[f // 4, f % 4]
        return 0

    with scope("widen"):
        lax.fori_loop(0, 16, widen, 0)

    def middle(b, size):
        if size >= 8:
            v = b.reshape(BLK // (2 * size), 2 * size, 2 * DK)[:, size - 1 : size, :]
            return jnp.broadcast_to(v, (BLK // (2 * size), 2 * size, 2 * DK)).reshape(BLK, 2 * DK)
        v = b.reshape(BLK // 8, 8, 2 * DK)
        sub = lax.broadcasted_iota(jnp.int32, (BLK // 8, 8, 2 * DK), 1)
        out = None
        for seg in range(8 // (2 * size)):
            at = seg * 2 * size + size - 1
            here = jnp.broadcast_to(v[:, at : at + 1, :], (BLK // 8, 8, 2 * DK))
            out = here if out is None else jnp.where(sub >= seg * 2 * size, here, out)
        return out.reshape(BLK, 2 * DK)

    def within(pair):
        spans = [pl.ds(pl.multiple_of((pair + n) * BLK, BLK), BLK) for n in range(2)]
        p = [proj[rows, :] for rows in spans]
        qk = [one[:, 0 : 2 * DK].astype(F32) for one in p]
        left = lax.broadcasted_iota(jnp.int32, (BLK, 2 * DK), 1) < DK
        q = jnp.where(left, qk[0], pltpu.roll(qk[1], DK, 1)) * DK**-0.5
        k = jnp.where(left, pltpu.roll(qk[0], DK, 1), qk[1])
        pre = [dot(one[:, PROJ : PROJ + GR], du2[...]) for one in p]
        pre = jnp.where(left, pre[0], pre[1]) + bias2[...]
        lg = (jnp.minimum(pre, 0.0) - jnp.log1p(jnp.exp(-jnp.abs(pre)))) / GATE_DIVISOR
        lev = level[...]
        tri = (lev >= 0).astype(BF16)
        b = jnp.zeros((BLK, 2 * DK), F32)
        for _ in range(3):
            top = lg.astype(BF16)
            b = b + dot(tri, top)
            lg = lg - top.astype(F32)

        def halves_of(values):
            values = values.astype(BF16)
            zero = jnp.zeros_like(values)
            return [jnp.where(left, values, zero), jnp.where(left, zero, values)]

        scores = None
        for n in range(8):
            if n:
                e = jnp.exp(-jnp.abs(b - middle(b, 2 ** (n - 1))))
                s = dot(jnp.concatenate(halves_of(q * e), axis=0), (k * e).astype(BF16), NT)
                scores = [jnp.where(lev == n, s[m * BLK : (m + 1) * BLK], scores[m]) for m in range(2)]
            else:
                s = dot(jnp.concatenate(halves_of(q), axis=0), k.astype(BF16), NT)
                scores = [jnp.where(lev == 0, s[m * BLK : (m + 1) * BLK], 0.0) for m in range(2)]
        last = b[BLK - 1 : BLK, :]
        carry = (k * jnp.exp(last - b)).astype(BF16)
        ends = halves_of(q * jnp.exp(b))
        fade = jnp.exp(jnp.broadcast_to(last, (8, 2 * DK)))
        for m in range(2):
            v = p[m][:, 128:256]
            inner[spans[m], :] = dot(scores[m].astype(BF16), v)
            qe[pair + m] = ends[m]
            both = [dot(v, carry, TN), fade]
            both = [
                jnp.where(lax.broadcasted_iota(jnp.int32, one.shape, 1) < DK, *((one, pltpu.roll(one, DK, 1))[:: 1 - 2 * m]))
                for one in both
            ]
            upd[pair + m] = both[0]
            shrink[pair + m] = both[1]
            gate[spans[m], :] = silu(p[m][:, 256:384].astype(F32)) * gain_ref[...]

    def arrived(block, slot):
        shared(block, slot).wait_recv()

    def project(pair):
        with scope("project"):
            rows = fa[pl.ds(pair, 2)].reshape(2 * ROWS, D)
            proj[pl.ds(pl.multiple_of(pair * ROWS, 256), 256), 0 : PROJ + GR] = dot(rows, WaW[...], NT).astype(BF16)
        with scope("within"):
            within(pair)

    arrived(t + 1 - 2 * c, 0)
    project(y * 2)
    with scope("rows1"):
        for way in (0, 1):
            along(side[way] + c, 1 - way, 1, way).wait_recv()
            share(side[way] + c, 1 - way, 1 + way)
            pending.append(shared(side[way] + c, 1 + way))
    with scope("rows1b"):
        arrived(side[0] + 1 - c, 1)
    project(side[0])
    with scope("rows2"):
        arrived(side[1] + 1 - c, 2)
    project(side[1])
    with scope("attention5"):
        each(gw, "pass_on", 2)
    with scope("rows2b"):
        for way in (0, 1):
            along(far + c, way, 2, way).wait_recv()
            share(far + c, way, 3)
        pending.append(shared(far + c, 3))
    with scope("rows3"):
        arrived(far + 1 - c, 3)
    project(far)

    def home(to):
        return pltpu.make_async_remote_copy(
            src_ref=gout.at[pl.ds(to * 256, 256)], dst_ref=gin.at[y],
            send_sem=hsend.at[to], recv_sem=hrecv.at[y],
            device_id=(r, zl * 4 + x, to * 2 + c), device_id_type=MESH,
        )

    state = jnp.zeros((DV, 2 * DK), F32)
    with scope("scan"):
        for i in range(8):
            rows = pl.ds(i * BLK, BLK)
            mixed = inner[rows, :] + dot(qe[i], state.astype(BF16), NT)
            state = state * shrink[i, 0:1] + upd[i]
            spread = jnp.mean(mixed * mixed, -1, keepdims=True)
            gout[rows, :] = (mixed * lax.rsqrt(spread + HEAD_EPS) * gate[rows, :]).astype(BF16)
            if i % 2:

                @pl.when(y != i // 2)
                def _():
                    home(i // 2).start()

                @pl.when(y == i // 2)
                def _():
                    gin[i // 2] = gout[(i - 1) * BLK : (i + 1) * BLK, :]

    with scope("wo"):
        each(gw, "finish", 2)
    settle()
    with scope("home"):
        for step in range(1, 4):
            source = (y + step) % 4
            pltpu.make_async_remote_copy(
                src_ref=gout.at[pl.ds(0, 256)], dst_ref=gin.at[source],
                send_sem=hsend.at[source], recv_sem=hrecv.at[source],
                device_id=(r, zl * 4 + x, source * 2 + c), device_id_type=MESH,
            ).wait()

    def out_proj(j, who):
        weights = jnp.concatenate(
            [jnp.concatenate([Wo[yy, j // 2, (j % 2) * 2 + i] for i in range(2)], axis=1) for yy in range(4)],
            axis=0,
        )
        rows = jnp.concatenate([gin[yy, rows_of(who)] for yy in range(4)], axis=1)
        acc[who, :, column_block(j)] = dot(rows, weights)

    with scope("outp"):
        pieces(out_proj, 1)
    second = joined(1, fa[t], RESIDUAL_SCALE, 1.0, 1)
    xs[...] = second


    def hand(piece):
        ref = xb.at[c, pl.ds(piece * 1024, 1024)]
        return across(ref, ref, 1)

    for piece in range(2):
        span = slice(piece * 1024, (piece + 1) * 1024)
        xb[c, span] = second[:, span].astype(F32).T.astype(BF16)
        hand(piece).start()
    both = across(xb.at[c], xb.at[c], 1)
    pending.append(both)
    with scope("swapx"):
        both.wait_recv()
    settle()
    for span in SECOND:
        ffn_compute(span, xb, 2)
    out_ref[...] = joined(2, xs[...], RESIDUAL_SCALE, BRANCH_SCALE, 2)
    if stop == 1:
        out_ref[...] = fa[t]
    if stop == 2:
        out_ref[...] = xs[...]
    settle()
    for phase in range(3):
        for g in ffn[0]:
            g.sent(phase, 0, HID)
        for g in gw + (ga if phase < 2 else []):
            g.sent(phase, g.rows[0], g.rows[2])


def on_device(
    stop, stream, gate_weight, up_weight, down_weight, query_weight, key_weight, value_weight, outgate_weight,
    decay_down, decay_up, decay_bias, head_gain, out_weight, norm_gain,
):
    vmem, hbm = (pl.BlockSpec(memory_space=space) for space in (pltpu.VMEM, pltpu.HBM))
    dma = pltpu.SemaphoreType.DMA
    return pl.pallas_call(
        functools.partial(kernel, stop),
        out_shape=jax.ShapeDtypeStruct((ROWS, D), BF16),
        in_specs=[hbm] * 9 + [vmem] * 3 + [hbm, vmem],
        out_specs=vmem,
        scratch_shapes=[
            pltpu.VMEM((ROWS, D), BF16),
            pltpu.VMEM((DK, 128), BF16),
            pltpu.VMEM((DK, 128), BF16),
            pltpu.VMEM((128, DV), BF16),
            pltpu.VMEM((128, DV), BF16),
            pltpu.VMEM((3, 4, 4, 4, HID, 128), BF16),
            pltpu.VMEM((4, 4, PROJ, 128), BF16),
            pltpu.VMEM((4, 4, 4, 128, 128), BF16),
            pltpu.VMEM((PROJ + GR, D), BF16),
            pltpu.VMEM((2, D, ROWS), BF16),
            pltpu.VMEM((2, D, ROWS), BF16),
            pltpu.VMEM((ROWS, D), BF16),
            pltpu.VMEM((4 * HID, 256), F32),
            pltpu.VMEM((256, 4 * HID), BF16),
            pltpu.VMEM((2, ROWS, D), F32),
            pltpu.VMEM((3, ROWS, D), F32),
            pltpu.VMEM((8, ROWS, D), BF16),
            pltpu.VMEM((1024, 512), BF16),
            pltpu.VMEM((1024, DV), F32),
            pltpu.VMEM((8, BLK, 2 * DK), BF16),
            pltpu.VMEM((8, DV, 2 * DK), F32),
            pltpu.VMEM((8, 8, 2 * DK), F32),
            pltpu.VMEM((1024, DV), F32),
            pltpu.VMEM((GR, 2 * DK), BF16),
            pltpu.VMEM((1, 2 * DK), F32),
            pltpu.VMEM((BLK, BLK), jnp.int32),
            pltpu.VMEM((1024, DV), BF16),
            pltpu.VMEM((4, 256, DV), BF16),
            dma((10,)),
            dma((3, 3)),
            dma((3, 3, 3, 2)),
            dma((2, 2)),
            dma((2, 2, 2)),
            dma((2, 3)),
            dma((2, 3, 2)),
            dma((9,)),
            dma((9,)),
            dma((3, 2)),
            dma((3, 2)),
            dma((4,)),
            dma((4,)),
        ],
        compiler_params=pltpu.CompilerParams(
            collective_id=0, has_side_effects=True, vmem_limit_bytes=VMEM_LIMIT
        ),
    )(
        stream, gate_weight.T, up_weight.T, down_weight, query_weight.T, key_weight.T, value_weight, outgate_weight,
        decay_down.T, decay_up, decay_bias[None], head_gain[None], out_weight, norm_gain,
    )


def solution(mesh, stop=0):
    in_specs = (
        P(("rep", "fs", "tp"), None),
        P("fs", "tp"),
        P("fs", "tp"),
        P("tp", "fs"),
        P("fs", "tp"),
        P("fs", "tp"),
        P("fs", "tp"),
        P("fs", "tp"),
        P(),
        P(None, "tp"),
        P("tp"),
        P(),
        P("tp", "fs"),
        P(),
    )
    return jax.shard_map(
        functools.partial(on_device, stop),
        mesh=mesh,
        in_specs=in_specs,
        out_specs=P(("rep", "fs", "tp"), None),
        check_vma=False,
    )
```

```python
import functools

import jax
import jax.numpy as jnp
from jax import lax
from jax.experimental import pallas as pl
from jax.experimental.pallas import tpu as pltpu
from jax.sharding import PartitionSpec as P

MESH = pl.DeviceIdType.MESH
F32, BF16 = jnp.float32, jnp.bfloat16
D, DK, DV, GR = 2048, 64, 128, 32
ROWS = 128
HID = 352
CHUNKS = ((0, 32, 64), (64, 160, 256), (256, 304, 352))
SECOND = ((0, HID),)
PROJ = 384
DIRECT = True
VMEM_LIMIT = 60 * 1024 * 1024
BLK = 128
RESIDUAL_SCALE = 2.0**0.5
BRANCH_SCALE = 0.5
NORM_EPS = 1e-05
HEAD_EPS = 0.01
GATE_DIVISOR = 16.0

NT = (((1,), (1,)), ((), ()))
NN = (((1,), (0,)), ((), ()))
TN = (((0,), (0,)), ((), ()))


def dot(a, b, dims=NN, **kw):
    return lax.dot_general(a, b, dims, preferred_element_type=F32, **kw)


def place():
    r, f, t = lax.axis_index("rep"), lax.axis_index("fs"), lax.axis_index("tp")
    return r, f // 4, f % 4, t // 2, t % 2


def neighbour(dim, step):
    r, zl, x, y, c = place()
    if dim == "x":
        return (r, zl * 4 + (x + step + 4) % 4, y * 2 + c)
    if dim == "y":
        return (r, zl * 4 + x, ((y + step + 4) % 4) * 2 + c)
    if dim == "c":
        return (r, zl * 4 + x, y * 2 + 1 - c)
    z = (r * 4 + zl + step + 8) % 8
    return (z // 4, (z % 4) * 4 + x, y * 2 + c)


class Gather:
    def __init__(self, order, at, rows, send, recv, direct=()):
        self.order, self.at, self.rows = order, at, rows
        self.send, self.recv, self.direct = send, recv, direct
        r, zl, x, y, c = place()
        self.pos = {"x": x, "y": y, "z": zl}

    def region(self, phase, along, lo, hi):
        idx = {}
        for k, dim in enumerate(self.order):
            if k < phase:
                idx[dim] = slice(None)
            elif k == phase:
                idx[dim] = along
            else:
                idx[dim] = self.pos[dim]
        return self.at(idx, pl.ds(lo, hi - lo))

    def copy(self, phase, region, late, step):
        return pltpu.make_async_remote_copy(
            src_ref=region,
            dst_ref=region,
            send_sem=self.send(phase),
            recv_sem=self.recv(phase, late),
            device_id=neighbour(self.order[phase], step),
            device_id_type=MESH,
        )

    def go(self, phase, shift, half, late, step):
        lo, mid, hi = self.rows
        lo, hi = ((lo, mid), (mid, hi))[half]
        self.copy(phase, self.region(phase, (self.pos[self.order[phase]] + shift) % 4, lo, hi), late, step).start()

    def whole(self, phase, count, late, lo, hi):
        return self.copy(phase, self.region(phase, pl.ds(0, count), lo, hi), late, 1)

    def begin(self, phase):
        for late in (0, 1):
            for way in (0, 1):
                self.go(phase, 0, way ^ late, late, 1 - 2 * way)
        if phase in self.direct:
            for way in (0, 1):
                self.go(phase, 0, way, 1, 2 - 4 * way)

    def first_halves(self, phase):
        self.whole(phase, 1, 0, self.rows[0], self.rows[2]).wait_recv()

    def pass_on(self, phase):
        if phase not in self.direct:
            self.first_halves(phase)
            for way in (0, 1):
                self.go(phase, 3 - 2 * way, way, 1, 1 - 2 * way)

    def finish(self, phase):
        if phase in self.direct:
            self.first_halves(phase)
        self.whole(phase, 2, 1, self.rows[0], self.rows[2]).wait_recv()

    def sent(self, phase, lo, hi):
        self.whole(phase, 3, 0, lo, hi).wait_send()


def layer_norm(values, norm_scale):
    average = jnp.mean(values, -1, keepdims=True)
    centred = values - average
    spread = jnp.mean(centred * centred, -1, keepdims=True)
    return (centred * lax.rsqrt(spread + NORM_EPS) * norm_scale).astype(BF16)


scope = jax.named_scope


def column_block(j):
    return pl.ds(j * 256 if isinstance(j, int) else pl.multiple_of(j * 256, 256), 256)


def silu(v):
    return v / (1.0 + jnp.exp(-v))


def kernel(
    stop,
    x_hbm, g_ref, u_ref, d_ref, q_hbm, k_hbm, v_hbm, og_hbm, dd_hbm, du_ref, bias_ref, gain_ref, wo_ref, norm_ref,
    out_ref,
    x_ref, q_ref, k_ref, v_ref, og_ref, W, Wa, Wo, WaW, xa, xb, xs, hidT, hid, acc, part, fa, proj, inner, qe, upd, shrink, states, gate, du2, bias2, level,
    gout, gin,
    lsem, fsend, frecv, asend, arecv, osend, orecv, csend, crecv, ysend, yrecv, hsend, hrecv,
):
    r, zl, x, y, c = place()
    t = y * 2 + c
    barrier = pltpu.get_barrier_semaphore()
    for dim in "xyz":
        for step in (1, -1, 2, -2) if dim == "z" else (1, -1, 2):
            pl.semaphore_signal(barrier, 1, device_id=neighbour(dim, step), device_id_type=MESH)
    for step in range(4):
        pl.semaphore_signal(barrier, 1, device_id=(r, zl * 4 + x, ((y + step) % 4) * 2 + 1 - c), device_id_type=MESH)
    own = []
    for w, ref in enumerate((g_ref, u_ref, d_ref)):
        own.append(pltpu.make_async_copy(ref, W.at[w, y, zl, x], lsem.at[w]))
    later = [pltpu.make_async_copy(wo_ref, Wo.at[c, y, zl, x], lsem.at[3])]
    for src, dst in (
        (q_hbm, q_ref),
        (k_hbm, k_ref),
        (v_hbm, v_ref),
        (og_hbm, og_ref),
        (dd_hbm, WaW.at[PROJ : PROJ + GR]),
        (x_hbm, x_ref),
    ):
        later.append(pltpu.make_async_copy(src, dst, lsem.at[3 + len(later)]))
    for cp in own + later:
        cp.start()
    with scope("barrier"):
        pl.semaphore_wait(barrier, 14)
        for cp in own:
            cp.wait()

    pending = []

    def go(cp):
        cp.start()
        pending.append(cp)

    def settle():
        for cp in pending:
            cp.wait_send()
        pending.clear()

    def across(src, dst, slot):
        return pltpu.make_async_remote_copy(
            src_ref=src, dst_ref=dst, send_sem=csend.at[slot], recv_sem=crecv.at[slot],
            device_id=neighbour("c", 1), device_id_type=MESH,
        )

    orders = (("x", "z", "y"), ("z", "y", "x"), ("y", "x", "z"))

    def ffn_gather(ch, w):
        return Gather(
            orders[w],
            lambda idx, rows: W.at[w, idx["y"], idx["z"], idx["x"], rows],
            CHUNKS[ch],
            lambda ph: fsend.at[w, ph],
            lambda ph, late: frecv.at[ch, w, ph, late],
            (0,) if ch == 0 and DIRECT else (),
        )

    ffn = [[ffn_gather(ch, w) for w in range(3)] for ch in range(3)]
    ga = [
        Gather(
            order, lambda idx, rows: Wa.at[idx["z"], idx["x"], rows], span,
            lambda ph, n=n: asend.at[n, ph], lambda ph, late, n=n: arecv.at[n, ph, late],
        )
        for n, (order, span) in enumerate(((("x", "z"), (0, 96, 192)), (("z", "x"), (192, 288, 384))))
    ]
    gw = [
        Gather(
            order, lambda idx, rows: Wo.at[c, idx["y"], idx["z"], idx["x"], rows], span,
            lambda ph, n=n: osend.at[n, ph], lambda ph, late, n=n: orecv.at[n, ph, late],
        )
        for n, (order, span) in enumerate(((("y", "x", "z"), (0, 32, 64)), (("y", "z", "x"), (64, 96, 128))))
    ]

    def each(gathers, op, phase):
        for g in gathers:
            getattr(g, op)(phase)

    def begin(ch, ph):
        with scope(f"begin{ch}_{ph}"):
            for w in range(3):
                if ph:
                    ffn[ch][w].finish(ph - 1)
                ffn[ch][w].begin(ph)

    def pass_on(ch, ph):
        with scope(f"pass{ch}_{ph}"):
            for w in range(3):
                ffn[ch][w].pass_on(ph)

    def hidden(lo, hi, rows):
        size = hi - lo

        def body(yy, _):
            both = [
                jnp.concatenate([W[w, yy, f // 4, f % 4, lo:hi, :] for f in range(16)], axis=1) for w in (0, 1)
            ]
            if size < 128:
                both = [jnp.concatenate(both, axis=0)]
            wide = jnp.concatenate([rows[0], rows[1]], axis=1)
            products = [dot(one, wide) for one in both]
            gate = products[0][:size]
            up = products[-1][-size:]
            hidT[pl.ds(pl.multiple_of(yy * size, 16), size), :] = silu(gate) * up
            return 0

        lax.fori_loop(0, 4, body, 0, unroll=True)
        hid[:, : 4 * size] = hidT[: 4 * size, :].T.astype(BF16)

    def down(lo, hi, slot):
        size = hi - lo

        def weights(j):
            return jnp.concatenate(
                [
                    jnp.concatenate([W[2, yy, j // 2, (j % 2) * 2 + i, lo:hi, :] for i in range(2)], axis=1)
                    for yy in range(4)
                ],
                axis=0,
            )

        def body(j, _):
            term = dot(hid[:, : 4 * size], weights(j))
            for half in range(2):
                piece = term[half * ROWS : (half + 1) * ROWS]
                if lo:
                    acc[half, :, column_block(j)] += piece
                else:
                    acc[half, :, column_block(j)] = piece
            return 0

        def one(j, who):
            term = dot(hid[rows_of(who), : 4 * size], weights(j))
            if lo:
                acc[who, :, column_block(j)] += term
            else:
                acc[who, :, column_block(j)] = term

        if hi == HID:
            pieces(one, slot)
        else:
            lax.fori_loop(0, 8, body, 0, unroll=2)

    def rows_of(who):
        return pl.ds(pl.multiple_of(who * ROWS, ROWS), ROWS)

    def give(slot, piece):
        cols = pl.ds(piece * 512, 512)
        return across(acc.at[1 - c, :, cols], part.at[slot, :, cols], 2 + slot)

    def given(slot):
        return across(acc.at[1 - c], part.at[slot], 2 + slot)

    def pieces(one, slot):
        for piece in range(4):
            for j in range(piece * 2, piece * 2 + 2):
                one(j, 1 - c)
            give(slot, piece).start()
        pending.append(given(slot))
        for j in range(8):
            one(j, c)

    def joined(slot, residual, scale, branch, norm):
        with scope(f"swap_{slot}"):
            given(slot).wait_recv()
        with scope(f"norm_{slot}"):
            total = acc[c] + part[slot]
            return layer_norm(scale * residual.astype(F32) + branch * total, norm_ref[norm : norm + 1, :])

    for ch in range(3):
        begin(ch, 0)
    for cp in later:
        cp.wait()
    Wa[zl, x, 0:64, :] = q_ref[...]
    Wa[zl, x, 64:128, :] = k_ref[...]
    Wa[zl, x, 128:256, :] = v_ref[...].astype(F32).T.astype(BF16)
    Wa[zl, x, 256:384, :] = og_ref[...].astype(F32).T.astype(BF16)
    pass_on(0, 0)
    pass_on(1, 0)
    begin(0, 1)
    pass_on(2, 0)
    begin(1, 1)
    each(ga, "begin", 0)
    each(gw, "begin", 0)
    pass_on(0, 1)
    begin(2, 1)
    begin(0, 2)
    pass_on(1, 1)
    each(ga, "pass_on", 0)
    each(gw, "pass_on", 0)
    pass_on(2, 1)
    xa[c] = x_ref[...].astype(F32).T.astype(BF16)
    go(across(xa.at[c], xa.at[c], 0))
    pass_on(0, 2)
    begin(1, 2)
    for half in range(2):
        du2[:, half * DK : (half + 1) * DK] = du_ref[...]
        bias2[:, half * DK : (half + 1) * DK] = bias_ref[...]
    rowi = lax.broadcasted_iota(jnp.int32, (BLK, BLK), 0)
    coli = lax.broadcasted_iota(jnp.int32, (BLK, BLK), 1)
    differ = jnp.bitwise_xor(rowi, coli)
    bits = jnp.zeros((BLK, BLK), jnp.int32)
    for k in range(7):
        bits = bits + (differ >= 2**k).astype(jnp.int32)
    level[...] = jnp.where(rowi >= coli, bits, -1)

    def ffn_compute(span, rows, slot):
        with scope(f"hidden{span[0]}"):
            hidden(*span, rows)
        with scope(f"down{span[0]}"):
            down(*span, slot)

    def finish(ch):
        with scope(f"finish{ch}"):
            for w in range(3):
                ffn[ch][w].finish(2)

    across(xa.at[c], xa.at[c], 0).wait_recv()
    finish(0)
    ffn_compute((0, 64), xa, 0)
    pass_on(1, 2)
    begin(2, 2)
    finish(1)
    ffn_compute((64, 256), xa, 0)
    pass_on(2, 2)
    each(ga, "finish", 0)
    each(ga, "begin", 1)
    each(gw, "finish", 0)
    each(gw, "begin", 1)
    finish(2)
    ffn_compute((256, HID), xa, 0)
    fa[t] = joined(0, x_ref[...], RESIDUAL_SCALE, BRANCH_SCALE, 0)

    half_rows = (pl.ds(0, ROWS // 2), pl.ds(ROWS // 2, ROWS // 2))

    def along(block, half, stage, way):
        ref = fa.at[block, half_rows[half]]
        return pltpu.make_async_remote_copy(
            src_ref=ref, dst_ref=ref, send_sem=ysend.at[stage, way], recv_sem=yrecv.at[stage, way],
            device_id=neighbour("y", 1 - 2 * way), device_id_type=MESH,
        )

    for stage in (0, 1):
        for way in (0, 1):
            go(along(t, way ^ stage, stage, way))

    def share(block, half, slot):
        ref = fa.at[block, half_rows[half]]
        across(ref, ref, 5 + slot).start()

    def shared(block, slot):
        return across(fa.at[block], fa.at[block], 5 + slot)

    go(shared(t, 0))
    side = [((y + 3) % 4) * 2, ((y + 1) % 4) * 2]
    far = ((y + 2) % 4) * 2

    with scope("attention2"):
        each(ga, "pass_on", 1)
    with scope("attention2b"):
        each(gw, "pass_on", 1)
    with scope("attention4"):
        each(gw, "finish", 1)
        each(gw, "begin", 2)
    with scope("rows0"):
        for way in (0, 1):
            along(side[way] + c, way, 0, way).wait_recv()
            go(along(side[way] + c, way, 2, way))
            share(side[way] + c, way, 1 + way)
    with scope("attention3"):
        each(ga, "finish", 1)

    def widen(f, _):
        WaW[0:PROJ, pl.ds(pl.multiple_of(f * 128, 128), 128)] = Wa[f // 4, f % 4]
        return 0

    with scope("widen"):
        lax.fori_loop(0, 16, widen, 0)

    def middle(b, size):
        if size >= 8:
            v = b.reshape(BLK // (2 * size), 2 * size, 2 * DK)[:, size - 1 : size, :]
            return jnp.broadcast_to(v, (BLK // (2 * size), 2 * size, 2 * DK)).reshape(BLK, 2 * DK)
        v = b.reshape(BLK // 8, 8, 2 * DK)
        sub = lax.broadcasted_iota(jnp.int32, (BLK // 8, 8, 2 * DK), 1)
        out = None
        for seg in range(8 // (2 * size)):
            at = seg * 2 * size + size - 1
            here = jnp.broadcast_to(v[:, at : at + 1, :], (BLK // 8, 8, 2 * DK))
            out = here if out is None else jnp.where(sub >= seg * 2 * size, here, out)
        return out.reshape(BLK, 2 * DK)

    def within(pair):
        spans = [pl.ds(pl.multiple_of((pair + n) * BLK, BLK), BLK) for n in range(2)]
        p = [proj[rows, :] for rows in spans]
        qk = [one[:, 0 : 2 * DK].astype(F32) for one in p]
        left = lax.broadcasted_iota(jnp.int32, (BLK, 2 * DK), 1) < DK
        q = jnp.where(left, qk[0], pltpu.roll(qk[1], DK, 1)) * DK**-0.5
        k = jnp.where(left, pltpu.roll(qk[0], DK, 1), qk[1])
        pre = [dot(one[:, PROJ : PROJ + GR], du2[...]) for one in p]
        pre = jnp.where(left, pre[0], pre[1]) + bias2[...]
        lg = (jnp.minimum(pre, 0.0) - jnp.log1p(jnp.exp(-jnp.abs(pre)))) / GATE_DIVISOR
        lev = level[...]
        tri = (lev >= 0).astype(BF16)
        b = jnp.zeros((BLK, 2 * DK), F32)
        for _ in range(3):
            top = lg.astype(BF16)
            b = b + dot(tri, top)
            lg = lg - top.astype(F32)

        def halves_of(values):
            values = values.astype(BF16)
            zero = jnp.zeros_like(values)
            return [jnp.where(left, values, zero), jnp.where(left, zero, values)]

        scores = None
        for n in range(8):
            if n:
                e = jnp.exp(-jnp.abs(b - middle(b, 2 ** (n - 1))))
                s = dot(jnp.concatenate(halves_of(q * e), axis=0), (k * e).astype(BF16), NT)
                scores = [jnp.where(lev == n, s[m * BLK : (m + 1) * BLK], scores[m]) for m in range(2)]
            else:
                s = dot(jnp.concatenate(halves_of(q), axis=0), k.astype(BF16), NT)
                scores = [jnp.where(lev == 0, s[m * BLK : (m + 1) * BLK], 0.0) for m in range(2)]
        last = b[BLK - 1 : BLK, :]
        carry = (k * jnp.exp(last - b)).astype(BF16)
        ends = halves_of(q * jnp.exp(b))
        fade = jnp.exp(jnp.broadcast_to(last, (8, 2 * DK)))
        for m in range(2):
            v = p[m][:, 128:256]
            inner[spans[m], :] = dot(scores[m].astype(BF16), v)
            qe[pair + m] = ends[m]
            both = [dot(v, carry, TN), fade]
            both = [
                jnp.where(lax.broadcasted_iota(jnp.int32, one.shape, 1) < DK, *((one, pltpu.roll(one, DK, 1))[:: 1 - 2 * m]))
                for one in both
            ]
            upd[pair + m] = both[0]
            shrink[pair + m] = both[1]
            gate[spans[m], :] = silu(p[m][:, 256:384].astype(F32)) * gain_ref[...]

    def arrived(block, slot):
        shared(block, slot).wait_recv()

    def project_one(block):
        proj[rows_of(block), 0 : PROJ + GR] = dot(fa[block], WaW[...], NT).astype(BF16)

    def project(pair):
        with scope("project"):
            rows = fa[pl.ds(pair, 2)].reshape(2 * ROWS, D)
            proj[pl.ds(pl.multiple_of(pair * ROWS, 256), 256), 0 : PROJ + GR] = dot(rows, WaW[...], NT).astype(BF16)
        with scope("within"):
            within(pair)

    arrived(t + 1 - 2 * c, 0)
    project(y * 2)
    with scope("rows1"):
        for way in (0, 1):
            along(side[way] + c, 1 - way, 1, way).wait_recv()
            share(side[way] + c, 1 - way, 1 + way)
            pending.append(shared(side[way] + c, 1 + way))
    with scope("attention5"):
        each(gw, "pass_on", 2)
    with scope("rows1b"):
        arrived(side[0] + 1 - c, 1)
    project(side[0])
    with scope("rows2"):
        arrived(side[1] + 1 - c, 2)
    project(side[1])
    with scope("rows2b"):
        for way in (0, 1):
            along(far + c, way, 2, way).wait_recv()
            share(far + c, way, 3)
        pending.append(shared(far + c, 3))
    project_one(far + c)
    with scope("rows3"):
        arrived(far + 1 - c, 3)
    project_one(far + 1 - c)
    with scope("wo"):
        each(gw, "finish", 2)
    go(across(Wo.at[c], Wo.at[c], 9))
    with scope("within"):
        within(far)

    def home(step, other):
        to = (y + step) % 4
        core = c + other - 2 * c * other
        return pltpu.make_async_remote_copy(
            src_ref=gout.at[rows_of(to * 2 + core)], dst_ref=gin.at[t],
            send_sem=hsend.at[step, other], recv_sem=hrecv.at[step, other],
            device_id=(r, zl * 4 + x, to * 2 + core), device_id_type=MESH,
        )

    state = jnp.zeros((DV, 2 * DK), F32)
    with scope("scan"):
        for i in range(8):
            states[i] = state.astype(BF16)
            state = state * shrink[i, 0:1] + upd[i]
        for step in (2, 1, 3, 0):
            to = (y + step) % 4
            for m in range(2):
                i = to * 2 + m
                rows = pl.ds(pl.multiple_of(i * BLK, BLK), BLK)
                mixed = inner[rows, :] + dot(qe[i], states[i], NT)
                spread = jnp.mean(mixed * mixed, -1, keepdims=True)
                done = (mixed * lax.rsqrt(spread + HEAD_EPS) * gate[rows, :]).astype(BF16)
                gout[rows, :] = done
            for other in range(2):
                if step or other:
                    go(home(step, other))
        gin[t] = gout[rows_of(t), :]

    with scope("home"):
        for step in (0, 1, 3, 2):
            for other in range(2):
                if step or other:
                    home(step, other).wait_recv()
    with scope("wo2"):
        across(Wo.at[1 - c], Wo.at[1 - c], 9).wait_recv()

    settle()
    with scope("outp"):
        rows = jnp.concatenate([gin[head] for head in range(8)], axis=1)
        for j in range(8):
            weights = jnp.concatenate(
                [
                    jnp.concatenate([Wo[head % 2, head // 2, j // 2, (j % 2) * 2 + i] for i in range(2)], axis=1)
                    for head in range(8)
                ],
                axis=0,
            )
            acc[c, :, column_block(j)] = dot(rows, weights)
    with scope("norm_1"):
        second = layer_norm(RESIDUAL_SCALE * fa[t].astype(F32) + acc[c], norm_ref[1:2, :])
    xs[...] = second


    def hand(piece):
        ref = xb.at[c, pl.ds(piece * 1024, 1024)]
        return across(ref, ref, 1)

    for piece in range(2):
        span = slice(piece * 1024, (piece + 1) * 1024)
        xb[c, span] = second[:, span].astype(F32).T.astype(BF16)
        hand(piece).start()
    both = across(xb.at[c], xb.at[c], 1)
    pending.append(both)
    with scope("swapx"):
        both.wait_recv()
    settle()
    for span in SECOND:
        ffn_compute(span, xb, 2)
    out_ref[...] = joined(2, xs[...], RESIDUAL_SCALE, BRANCH_SCALE, 2)
    if stop == 1:
        out_ref[...] = fa[t]
    if stop == 2:
        out_ref[...] = xs[...]
    settle()
    for phase in range(3):
        for g in ffn[0]:
            g.sent(phase, 0, HID)
        for g in gw + (ga if phase < 2 else []):
            g.sent(phase, g.rows[0], g.rows[2])


def on_device(
    stop, stream, gate_weight, up_weight, down_weight, query_weight, key_weight, value_weight, outgate_weight,
    decay_down, decay_up, decay_bias, head_gain, out_weight, norm_gain,
):
    vmem, hbm = (pl.BlockSpec(memory_space=space) for space in (pltpu.VMEM, pltpu.HBM))
    dma = pltpu.SemaphoreType.DMA
    return pl.pallas_call(
        functools.partial(kernel, stop),
        out_shape=jax.ShapeDtypeStruct((ROWS, D), BF16),
        in_specs=[hbm] * 9 + [vmem] * 3 + [hbm, vmem],
        out_specs=vmem,
        scratch_shapes=[
            pltpu.VMEM((ROWS, D), BF16),
            pltpu.VMEM((DK, 128), BF16),
            pltpu.VMEM((DK, 128), BF16),
            pltpu.VMEM((128, DV), BF16),
            pltpu.VMEM((128, DV), BF16),
            pltpu.VMEM((3, 4, 4, 4, HID, 128), BF16),
            pltpu.VMEM((4, 4, PROJ, 128), BF16),
            pltpu.VMEM((2, 4, 4, 4, 128, 128), BF16),
            pltpu.VMEM((PROJ + GR, D), BF16),
            pltpu.VMEM((2, D, ROWS), BF16),
            pltpu.VMEM((2, D, ROWS), BF16),
            pltpu.VMEM((ROWS, D), BF16),
            pltpu.VMEM((4 * HID, 256), F32),
            pltpu.VMEM((256, 4 * HID), BF16),
            pltpu.VMEM((2, ROWS, D), F32),
            pltpu.VMEM((3, ROWS, D), F32),
            pltpu.VMEM((8, ROWS, D), BF16),
            pltpu.VMEM((1024, 512), BF16),
            pltpu.VMEM((1024, DV), F32),
            pltpu.VMEM((8, BLK, 2 * DK), BF16),
            pltpu.VMEM((8, DV, 2 * DK), F32),
            pltpu.VMEM((8, 8, 2 * DK), F32),
            pltpu.VMEM((8, DV, 2 * DK), BF16),
            pltpu.VMEM((1024, DV), F32),
            pltpu.VMEM((GR, 2 * DK), BF16),
            pltpu.VMEM((1, 2 * DK), F32),
            pltpu.VMEM((BLK, BLK), jnp.int32),
            pltpu.VMEM((1024, DV), BF16),
            pltpu.VMEM((8, ROWS, DV), BF16),
            dma((10,)),
            dma((3, 3)),
            dma((3, 3, 3, 2)),
            dma((2, 2)),
            dma((2, 2, 2)),
            dma((2, 3)),
            dma((2, 3, 2)),
            dma((10,)),
            dma((10,)),
            dma((3, 2)),
            dma((3, 2)),
            dma((4, 2)),
            dma((4, 2)),
        ],
        compiler_params=pltpu.CompilerParams(
            collective_id=0, has_side_effects=True, vmem_limit_bytes=VMEM_LIMIT
        ),
    )(
        stream, gate_weight.T, up_weight.T, down_weight, query_weight.T, key_weight.T, value_weight, outgate_weight,
        decay_down.T, decay_up, decay_bias[None], head_gain[None], out_weight, norm_gain,
    )


def solution(mesh, stop=0):
    in_specs = (
        P(("rep", "fs", "tp"), None),
        P("fs", "tp"),
        P("fs", "tp"),
        P("tp", "fs"),
        P("fs", "tp"),
        P("fs", "tp"),
        P("fs", "tp"),
        P("fs", "tp"),
        P(),
        P(None, "tp"),
        P("tp"),
        P(),
        P("tp", "fs"),
        P(),
    )
    return jax.shard_map(
        functools.partial(on_device, stop),
        mesh=mesh,
        in_specs=in_specs,
        out_specs=P(("rep", "fs", "tp"), None),
        check_vma=False,
    )
```

```python
import functools

import jax
import jax.numpy as jnp
from jax import lax
from jax.experimental import pallas as pl
from jax.experimental.pallas import tpu as pltpu
from jax.sharding import PartitionSpec as P

MESH = pl.DeviceIdType.MESH
F32, BF16 = jnp.float32, jnp.bfloat16
D, DK, DV, GR = 2048, 64, 128, 32
ROWS = 128
HID = 352
CHUNKS = ((0, 32, 64), (64, 176, 288), (288, 320, 352))
SECOND = ((0, HID),)
PROJ = 384
DIRECT = True
VMEM_LIMIT = 60 * 1024 * 1024
BLK = 128
RESIDUAL_SCALE = 2.0**0.5
BRANCH_SCALE = 0.5
NORM_EPS = 1e-05
HEAD_EPS = 0.01
GATE_DIVISOR = 16.0

NT = (((1,), (1,)), ((), ()))
NN = (((1,), (0,)), ((), ()))
TN = (((0,), (0,)), ((), ()))


def dot(a, b, dims=NN, **kw):
    return lax.dot_general(a, b, dims, preferred_element_type=F32, **kw)


def place():
    r, f, t = lax.axis_index("rep"), lax.axis_index("fs"), lax.axis_index("tp")
    return r, f // 4, f % 4, t // 2, t % 2


def neighbour(dim, step):
    r, zl, x, y, c = place()
    if dim == "x":
        return (r, zl * 4 + (x + step + 4) % 4, y * 2 + c)
    if dim == "y":
        return (r, zl * 4 + x, ((y + step + 4) % 4) * 2 + c)
    if dim == "c":
        return (r, zl * 4 + x, y * 2 + 1 - c)
    z = (r * 4 + zl + step + 8) % 8
    return (z // 4, (z % 4) * 4 + x, y * 2 + c)


class Gather:
    def __init__(self, order, at, rows, send, recv, direct=()):
        self.order, self.at, self.rows = order, at, rows
        self.send, self.recv, self.direct = send, recv, direct
        r, zl, x, y, c = place()
        self.pos = {"x": x, "y": y, "z": zl}

    def region(self, phase, along, lo, hi):
        idx = {}
        for k, dim in enumerate(self.order):
            if k < phase:
                idx[dim] = slice(None)
            elif k == phase:
                idx[dim] = along
            else:
                idx[dim] = self.pos[dim]
        return self.at(idx, pl.ds(lo, hi - lo))

    def copy(self, phase, region, late, step):
        return pltpu.make_async_remote_copy(
            src_ref=region,
            dst_ref=region,
            send_sem=self.send(phase),
            recv_sem=self.recv(phase, late),
            device_id=neighbour(self.order[phase], step),
            device_id_type=MESH,
        )

    def go(self, phase, shift, half, late, step):
        lo, mid, hi = self.rows
        lo, hi = ((lo, mid), (mid, hi))[half]
        self.copy(phase, self.region(phase, (self.pos[self.order[phase]] + shift) % 4, lo, hi), late, step).start()

    def whole(self, phase, count, late, lo, hi):
        return self.copy(phase, self.region(phase, pl.ds(0, count), lo, hi), late, 1)

    def begin(self, phase):
        for late in (0, 1):
            for way in (0, 1):
                self.go(phase, 0, way ^ late, late, 1 - 2 * way)
        if phase in self.direct:
            for way in (0, 1):
                self.go(phase, 0, way, 1, 2 - 4 * way)

    def first_halves(self, phase):
        self.whole(phase, 1, 0, self.rows[0], self.rows[2]).wait_recv()

    def pass_on(self, phase):
        if phase not in self.direct:
            self.first_halves(phase)
            for way in (0, 1):
                self.go(phase, 3 - 2 * way, way, 1, 1 - 2 * way)

    def finish(self, phase):
        if phase in self.direct:
            self.first_halves(phase)
        self.whole(phase, 2, 1, self.rows[0], self.rows[2]).wait_recv()

    def sent(self, phase, lo, hi):
        self.whole(phase, 3, 0, lo, hi).wait_send()


def layer_norm(values, norm_scale):
    average = jnp.mean(values, -1, keepdims=True)
    centred = values - average
    spread = jnp.mean(centred * centred, -1, keepdims=True)
    return (centred * lax.rsqrt(spread + NORM_EPS) * norm_scale).astype(BF16)


scope = jax.named_scope


def column_block(j):
    return pl.ds(j * 256 if isinstance(j, int) else pl.multiple_of(j * 256, 256), 256)


def silu(v):
    return v / (1.0 + jnp.exp(-v))


def kernel(
    stop,
    x_hbm, g_ref, u_ref, d_ref, q_hbm, k_hbm, v_hbm, og_hbm, dd_hbm, du_ref, bias_ref, gain_ref, wo_ref, norm_ref,
    out_ref,
    x_ref, q_ref, k_ref, v_ref, og_ref, W, Wa, Wo, WaW, xa, xb, xs, hidT, hid, acc, part, fa, proj, inner, qe, upd, shrink, states, gate, du2, bias2, level,
    gout, gin,
    lsem, fsend, frecv, asend, arecv, osend, orecv, csend, crecv, ysend, yrecv, hsend, hrecv,
):
    r, zl, x, y, c = place()
    t = y * 2 + c
    barrier = pltpu.get_barrier_semaphore()
    for dim in "xyz":
        for step in (1, -1, 2, -2) if dim == "z" else (1, -1, 2):
            pl.semaphore_signal(barrier, 1, device_id=neighbour(dim, step), device_id_type=MESH)
    for step in range(4):
        pl.semaphore_signal(barrier, 1, device_id=(r, zl * 4 + x, ((y + step) % 4) * 2 + 1 - c), device_id_type=MESH)
    own = []
    for w, ref in enumerate((g_ref, u_ref, d_ref)):
        own.append(pltpu.make_async_copy(ref, W.at[w, y, zl, x], lsem.at[w]))
    later = [pltpu.make_async_copy(wo_ref, Wo.at[c, y, zl, x], lsem.at[3])]
    for src, dst in (
        (q_hbm, q_ref),
        (k_hbm, k_ref),
        (v_hbm, v_ref),
        (og_hbm, og_ref),
        (dd_hbm, WaW.at[PROJ : PROJ + GR]),
        (x_hbm, x_ref),
    ):
        later.append(pltpu.make_async_copy(src, dst, lsem.at[3 + len(later)]))
    for cp in own + later:
        cp.start()
    with scope("barrier"):
        pl.semaphore_wait(barrier, 14)
        for cp in own:
            cp.wait()

    pending = []

    def go(cp):
        cp.start()
        pending.append(cp)

    def settle():
        for cp in pending:
            cp.wait_send()
        pending.clear()

    def across(src, dst, slot):
        return pltpu.make_async_remote_copy(
            src_ref=src, dst_ref=dst, send_sem=csend.at[slot], recv_sem=crecv.at[slot],
            device_id=neighbour("c", 1), device_id_type=MESH,
        )

    orders = (("x", "z", "y"), ("z", "y", "x"), ("y", "x", "z"))

    def ffn_gather(ch, w):
        return Gather(
            orders[w],
            lambda idx, rows: W.at[w, idx["y"], idx["z"], idx["x"], rows],
            CHUNKS[ch],
            lambda ph: fsend.at[w, ph],
            lambda ph, late: frecv.at[ch, w, ph, late],
            (0, 1) if ch == 0 and DIRECT else (),
        )

    ffn = [[ffn_gather(ch, w) for w in range(3)] for ch in range(3)]
    ga = [
        Gather(
            order, lambda idx, rows: Wa.at[idx["z"], idx["x"], rows], span,
            lambda ph, n=n: asend.at[n, ph], lambda ph, late, n=n: arecv.at[n, ph, late],
        )
        for n, (order, span) in enumerate(((("x", "z"), (0, 96, 192)), (("z", "x"), (192, 288, 384))))
    ]
    gw = [
        Gather(
            order, lambda idx, rows: Wo.at[c, idx["y"], idx["z"], idx["x"], rows], span,
            lambda ph, n=n: osend.at[n, ph], lambda ph, late, n=n: orecv.at[n, ph, late],
        )
        for n, (order, span) in enumerate(((("y", "x", "z"), (0, 32, 64)), (("y", "z", "x"), (64, 96, 128))))
    ]

    def each(gathers, op, phase):
        for g in gathers:
            getattr(g, op)(phase)

    def begin(ch, ph):
        with scope(f"begin{ch}_{ph}"):
            for w in range(3):
                if ph:
                    ffn[ch][w].finish(ph - 1)
                ffn[ch][w].begin(ph)

    def pass_on(ch, ph):
        with scope(f"pass{ch}_{ph}"):
            for w in range(3):
                ffn[ch][w].pass_on(ph)

    def hidden(lo, hi, rows):
        size = hi - lo

        def body(yy, _):
            both = [
                jnp.concatenate([W[w, yy, f // 4, f % 4, lo:hi, :] for f in range(16)], axis=1) for w in (0, 1)
            ]
            if size < 128:
                both = [jnp.concatenate(both, axis=0)]
            wide = jnp.concatenate([rows[0], rows[1]], axis=1)
            products = [dot(one, wide) for one in both]
            gate = products[0][:size]
            up = products[-1][-size:]
            hidT[pl.ds(pl.multiple_of(yy * size, 16), size), :] = silu(gate) * up
            return 0

        lax.fori_loop(0, 4, body, 0, unroll=True)
        hid[:, : 4 * size] = hidT[: 4 * size, :].T.astype(BF16)

    def down(lo, hi, slot):
        size = hi - lo

        def weights(j):
            return jnp.concatenate(
                [
                    jnp.concatenate([W[2, yy, j // 2, (j % 2) * 2 + i, lo:hi, :] for i in range(2)], axis=1)
                    for yy in range(4)
                ],
                axis=0,
            )

        def body(j, _):
            term = dot(hid[:, : 4 * size], weights(j))
            for half in range(2):
                piece = term[half * ROWS : (half + 1) * ROWS]
                if lo:
                    acc[half, :, column_block(j)] += piece
                else:
                    acc[half, :, column_block(j)] = piece
            return 0

        def one(j, who):
            term = dot(hid[rows_of(who), : 4 * size], weights(j))
            if lo:
                acc[who, :, column_block(j)] += term
            else:
                acc[who, :, column_block(j)] = term

        if hi == HID:
            pieces(one, slot)
        else:
            lax.fori_loop(0, 8, body, 0, unroll=2)

    def rows_of(who):
        return pl.ds(pl.multiple_of(who * ROWS, ROWS), ROWS)

    def give(slot, piece):
        cols = pl.ds(piece * 512, 512)
        return across(acc.at[1 - c, :, cols], part.at[slot, :, cols], 2 + slot)

    def given(slot):
        return across(acc.at[1 - c], part.at[slot], 2 + slot)

    def pieces(one, slot):
        for piece in range(4):
            for j in range(piece * 2, piece * 2 + 2):
                one(j, 1 - c)
            give(slot, piece).start()
        pending.append(given(slot))
        for j in range(8):
            one(j, c)

    def joined(slot, residual, scale, branch, norm):
        with scope(f"swap_{slot}"):
            given(slot).wait_recv()
        with scope(f"norm_{slot}"):
            total = acc[c] + part[slot]
            return layer_norm(scale * residual.astype(F32) + branch * total, norm_ref[norm : norm + 1, :])

    for ch in range(3):
        begin(ch, 0)
    for cp in later:
        cp.wait()
    Wa[zl, x, 0:64, :] = q_ref[...]
    Wa[zl, x, 64:128, :] = k_ref[...]
    Wa[zl, x, 128:256, :] = v_ref[...].astype(F32).T.astype(BF16)
    Wa[zl, x, 256:384, :] = og_ref[...].astype(F32).T.astype(BF16)
    pass_on(0, 0)
    pass_on(1, 0)
    begin(0, 1)
    pass_on(2, 0)
    begin(1, 1)
    each(ga, "begin", 0)
    each(gw, "begin", 0)
    pass_on(0, 1)
    begin(2, 1)
    begin(0, 2)
    pass_on(1, 1)
    each(ga, "pass_on", 0)
    each(gw, "pass_on", 0)
    pass_on(2, 1)
    xa[c] = x_ref[...].astype(F32).T.astype(BF16)
    go(across(xa.at[c], xa.at[c], 0))
    pass_on(0, 2)
    begin(1, 2)
    for half in range(2):
        du2[:, half * DK : (half + 1) * DK] = du_ref[...]
        bias2[:, half * DK : (half + 1) * DK] = bias_ref[...]
    rowi = lax.broadcasted_iota(jnp.int32, (BLK, BLK), 0)
    coli = lax.broadcasted_iota(jnp.int32, (BLK, BLK), 1)
    differ = jnp.bitwise_xor(rowi, coli)
    bits = jnp.zeros((BLK, BLK), jnp.int32)
    for k in range(7):
        bits = bits + (differ >= 2**k).astype(jnp.int32)
    level[...] = jnp.where(rowi >= coli, bits, -1)

    def ffn_compute(span, rows, slot):
        with scope(f"hidden{span[0]}"):
            hidden(*span, rows)
        with scope(f"down{span[0]}"):
            down(*span, slot)

    def finish(ch):
        with scope(f"finish{ch}"):
            for w in range(3):
                ffn[ch][w].finish(2)

    across(xa.at[c], xa.at[c], 0).wait_recv()
    finish(0)
    ffn_compute((0, 64), xa, 0)
    pass_on(1, 2)
    begin(2, 2)
    finish(1)
    ffn_compute((64, 288), xa, 0)
    pass_on(2, 2)
    each(ga, "finish", 0)
    each(ga, "begin", 1)
    each(gw, "finish", 0)
    each(gw, "begin", 1)
    finish(2)
    ffn_compute((288, HID), xa, 0)
    fa[t] = joined(0, x_ref[...], RESIDUAL_SCALE, BRANCH_SCALE, 0)

    half_rows = (pl.ds(0, ROWS // 2), pl.ds(ROWS // 2, ROWS // 2))

    def along(block, half, stage, way):
        ref = fa.at[block, half_rows[half]]
        return pltpu.make_async_remote_copy(
            src_ref=ref, dst_ref=ref, send_sem=ysend.at[stage, way], recv_sem=yrecv.at[stage, way],
            device_id=neighbour("y", 1 - 2 * way), device_id_type=MESH,
        )

    for stage in (0, 1):
        for way in (0, 1):
            go(along(t, way ^ stage, stage, way))

    def share(block, half, slot):
        ref = fa.at[block, half_rows[half]]
        across(ref, ref, 5 + slot).start()

    def shared(block, slot):
        return across(fa.at[block], fa.at[block], 5 + slot)

    go(shared(t, 0))
    side = [((y + 3) % 4) * 2, ((y + 1) % 4) * 2]
    far = ((y + 2) % 4) * 2

    with scope("attention2"):
        each(ga, "pass_on", 1)
    with scope("attention2b"):
        each(gw, "pass_on", 1)
    with scope("attention4"):
        each(gw, "finish", 1)
        each(gw, "begin", 2)
    with scope("rows0"):
        for way in (0, 1):
            along(side[way] + c, way, 0, way).wait_recv()
            go(along(side[way] + c, way, 2, way))
            share(side[way] + c, way, 1 + way)
    with scope("attention3"):
        each(ga, "finish", 1)

    def widen(f, _):
        WaW[0:PROJ, pl.ds(pl.multiple_of(f * 128, 128), 128)] = Wa[f // 4, f % 4]
        return 0

    with scope("widen"):
        lax.fori_loop(0, 16, widen, 0)

    def middle(b, size):
        if size >= 8:
            v = b.reshape(BLK // (2 * size), 2 * size, 2 * DK)[:, size - 1 : size, :]
            return jnp.broadcast_to(v, (BLK // (2 * size), 2 * size, 2 * DK)).reshape(BLK, 2 * DK)
        v = b.reshape(BLK // 8, 8, 2 * DK)
        sub = lax.broadcasted_iota(jnp.int32, (BLK // 8, 8, 2 * DK), 1)
        out = None
        for seg in range(8 // (2 * size)):
            at = seg * 2 * size + size - 1
            here = jnp.broadcast_to(v[:, at : at + 1, :], (BLK // 8, 8, 2 * DK))
            out = here if out is None else jnp.where(sub >= seg * 2 * size, here, out)
        return out.reshape(BLK, 2 * DK)

    def within(pair):
        spans = [pl.ds(pl.multiple_of((pair + n) * BLK, BLK), BLK) for n in range(2)]
        p = [proj[rows, :] for rows in spans]
        qk = [one[:, 0 : 2 * DK].astype(F32) for one in p]
        left = lax.broadcasted_iota(jnp.int32, (BLK, 2 * DK), 1) < DK
        q = jnp.where(left, qk[0], pltpu.roll(qk[1], DK, 1)) * DK**-0.5
        k = jnp.where(left, pltpu.roll(qk[0], DK, 1), qk[1])
        pre = [dot(one[:, PROJ : PROJ + GR], du2[...]) for one in p]
        pre = jnp.where(left, pre[0], pre[1]) + bias2[...]
        lg = (jnp.minimum(pre, 0.0) - jnp.log1p(jnp.exp(-jnp.abs(pre)))) / GATE_DIVISOR
        lev = level[...]
        tri = (lev >= 0).astype(BF16)
        b = jnp.zeros((BLK, 2 * DK), F32)
        for _ in range(3):
            top = lg.astype(BF16)
            b = b + dot(tri, top)
            lg = lg - top.astype(F32)

        def halves_of(values):
            values = values.astype(BF16)
            zero = jnp.zeros_like(values)
            return [jnp.where(left, values, zero), jnp.where(left, zero, values)]

        scores = None
        for n in range(8):
            if n:
                e = jnp.exp(-jnp.abs(b - middle(b, 2 ** (n - 1))))
                s = dot(jnp.concatenate(halves_of(q * e), axis=0), (k * e).astype(BF16), NT)
                scores = [jnp.where(lev == n, s[m * BLK : (m + 1) * BLK], scores[m]) for m in range(2)]
            else:
                s = dot(jnp.concatenate(halves_of(q), axis=0), k.astype(BF16), NT)
                scores = [jnp.where(lev == 0, s[m * BLK : (m + 1) * BLK], 0.0) for m in range(2)]
        last = b[BLK - 1 : BLK, :]
        carry = (k * jnp.exp(last - b)).astype(BF16)
        ends = halves_of(q * jnp.exp(b))
        fade = jnp.exp(jnp.broadcast_to(last, (8, 2 * DK)))
        for m in range(2):
            v = p[m][:, 128:256]
            inner[spans[m], :] = dot(scores[m].astype(BF16), v)
            qe[pair + m] = ends[m]
            both = [dot(v, carry, TN), fade]
            both = [
                jnp.where(lax.broadcasted_iota(jnp.int32, one.shape, 1) < DK, *((one, pltpu.roll(one, DK, 1))[:: 1 - 2 * m]))
                for one in both
            ]
            upd[pair + m] = both[0]
            shrink[pair + m] = both[1]
            gate[spans[m], :] = silu(p[m][:, 256:384].astype(F32)) * gain_ref[...]

    def arrived(block, slot):
        shared(block, slot).wait_recv()

    def project_one(block):
        proj[rows_of(block), 0 : PROJ + GR] = dot(fa[block], WaW[...], NT).astype(BF16)

    def project(pair):
        with scope("project"):
            rows = fa[pl.ds(pair, 2)].reshape(2 * ROWS, D)
            proj[pl.ds(pl.multiple_of(pair * ROWS, 256), 256), 0 : PROJ + GR] = dot(rows, WaW[...], NT).astype(BF16)
        with scope("within"):
            within(pair)

    arrived(t + 1 - 2 * c, 0)
    project(y * 2)
    with scope("rows1"):
        for way in (0, 1):
            along(side[way] + c, 1 - way, 1, way).wait_recv()
            share(side[way] + c, 1 - way, 1 + way)
            pending.append(shared(side[way] + c, 1 + way))
    with scope("attention5"):
        each(gw, "pass_on", 2)
    with scope("rows1b"):
        arrived(side[0] + 1 - c, 1)
    project(side[0])
    with scope("rows2"):
        arrived(side[1] + 1 - c, 2)
    project(side[1])
    with scope("rows2b"):
        for way in (0, 1):
            along(far + c, way, 2, way).wait_recv()
            share(far + c, way, 3)
        pending.append(shared(far + c, 3))
    project_one(far + c)
    with scope("rows3"):
        arrived(far + 1 - c, 3)
    project_one(far + 1 - c)
    with scope("wo"):
        each(gw, "finish", 2)
    go(across(Wo.at[c], Wo.at[c], 9))
    with scope("within"):
        within(far)

    def home(step, other):
        to = (y + step) % 4
        core = c + other - 2 * c * other
        return pltpu.make_async_remote_copy(
            src_ref=gout.at[rows_of(to * 2 + core)], dst_ref=gin.at[t],
            send_sem=hsend.at[step, other], recv_sem=hrecv.at[step, other],
            device_id=(r, zl * 4 + x, to * 2 + core), device_id_type=MESH,
        )

    state = jnp.zeros((DV, 2 * DK), F32)
    with scope("scan"):
        for i in range(8):
            states[i] = state.astype(BF16)
            state = state * shrink[i, 0:1] + upd[i]
        for step in (2, 1, 3, 0):
            to = (y + step) % 4
            for m in range(2):
                i = to * 2 + m
                rows = pl.ds(pl.multiple_of(i * BLK, BLK), BLK)
                mixed = inner[rows, :] + dot(qe[i], states[i], NT)
                spread = jnp.mean(mixed * mixed, -1, keepdims=True)
                done = (mixed * lax.rsqrt(spread + HEAD_EPS) * gate[rows, :]).astype(BF16)
                gout[rows, :] = done
            for other in range(2):
                if step or other:
                    go(home(step, other))
        gin[t] = gout[rows_of(t), :]

    with scope("home"):
        for step in (0, 1, 3, 2):
            for other in range(2):
                if step or other:
                    home(step, other).wait_recv()
    with scope("wo2"):
        across(Wo.at[1 - c], Wo.at[1 - c], 9).wait_recv()

    settle()
    with scope("outp"):
        rows = jnp.concatenate([gin[head] for head in range(8)], axis=1)
        for j in range(8):
            weights = jnp.concatenate(
                [
                    jnp.concatenate([Wo[head % 2, head // 2, j // 2, (j % 2) * 2 + i] for i in range(2)], axis=1)
                    for head in range(8)
                ],
                axis=0,
            )
            acc[c, :, column_block(j)] = dot(rows, weights)
    with scope("norm_1"):
        second = layer_norm(RESIDUAL_SCALE * fa[t].astype(F32) + acc[c], norm_ref[1:2, :])
    xs[...] = second


    def hand(piece):
        ref = xb.at[c, pl.ds(piece * 512, 512)]
        return across(ref, ref, 1)

    for piece in range(4):
        span = slice(piece * 512, (piece + 1) * 512)
        xb[c, span] = second[:, span].astype(F32).T.astype(BF16)
        hand(piece).start()
    both = across(xb.at[c], xb.at[c], 1)
    pending.append(both)
    with scope("swapx"):
        both.wait_recv()
    settle()
    for span in SECOND:
        ffn_compute(span, xb, 2)
    out_ref[...] = joined(2, xs[...], RESIDUAL_SCALE, BRANCH_SCALE, 2)
    if stop == 1:
        out_ref[...] = fa[t]
    if stop == 2:
        out_ref[...] = xs[...]
    settle()
    for phase in range(3):
        for g in ffn[0]:
            g.sent(phase, 0, HID)
        for g in gw + (ga if phase < 2 else []):
            g.sent(phase, g.rows[0], g.rows[2])


def on_device(
    stop, stream, gate_weight, up_weight, down_weight, query_weight, key_weight, value_weight, outgate_weight,
    decay_down, decay_up, decay_bias, head_gain, out_weight, norm_gain,
):
    vmem, hbm = (pl.BlockSpec(memory_space=space) for space in (pltpu.VMEM, pltpu.HBM))
    dma = pltpu.SemaphoreType.DMA
    return pl.pallas_call(
        functools.partial(kernel, stop),
        out_shape=jax.ShapeDtypeStruct((ROWS, D), BF16),
        in_specs=[hbm] * 9 + [vmem] * 3 + [hbm, vmem],
        out_specs=vmem,
        scratch_shapes=[
            pltpu.VMEM((ROWS, D), BF16),
            pltpu.VMEM((DK, 128), BF16),
            pltpu.VMEM((DK, 128), BF16),
            pltpu.VMEM((128, DV), BF16),
            pltpu.VMEM((128, DV), BF16),
            pltpu.VMEM((3, 4, 4, 4, HID, 128), BF16),
            pltpu.VMEM((4, 4, PROJ, 128), BF16),
            pltpu.VMEM((2, 4, 4, 4, 128, 128), BF16),
            pltpu.VMEM((PROJ + GR, D), BF16),
            pltpu.VMEM((2, D, ROWS), BF16),
            pltpu.VMEM((2, D, ROWS), BF16),
            pltpu.VMEM((ROWS, D), BF16),
            pltpu.VMEM((4 * HID, 256), F32),
            pltpu.VMEM((256, 4 * HID), BF16),
            pltpu.VMEM((2, ROWS, D), F32),
            pltpu.VMEM((3, ROWS, D), F32),
            pltpu.VMEM((8, ROWS, D), BF16),
            pltpu.VMEM((1024, 512), BF16),
            pltpu.VMEM((1024, DV), F32),
            pltpu.VMEM((8, BLK, 2 * DK), BF16),
            pltpu.VMEM((8, DV, 2 * DK), F32),
            pltpu.VMEM((8, 8, 2 * DK), F32),
            pltpu.VMEM((8, DV, 2 * DK), BF16),
            pltpu.VMEM((1024, DV), F32),
            pltpu.VMEM((GR, 2 * DK), BF16),
            pltpu.VMEM((1, 2 * DK), F32),
            pltpu.VMEM((BLK, BLK), jnp.int32),
            pltpu.VMEM((1024, DV), BF16),
            pltpu.VMEM((8, ROWS, DV), BF16),
            dma((10,)),
            dma((3, 3)),
            dma((3, 3, 3, 2)),
            dma((2, 2)),
            dma((2, 2, 2)),
            dma((2, 3)),
            dma((2, 3, 2)),
            dma((10,)),
            dma((10,)),
            dma((3, 2)),
            dma((3, 2)),
            dma((4, 2)),
            dma((4, 2)),
        ],
        compiler_params=pltpu.CompilerParams(
            collective_id=0, has_side_effects=True, vmem_limit_bytes=VMEM_LIMIT
        ),
    )(
        stream, gate_weight.T, up_weight.T, down_weight, query_weight.T, key_weight.T, value_weight, outgate_weight,
        decay_down.T, decay_up, decay_bias[None], head_gain[None], out_weight, norm_gain,
    )


def solution(mesh, stop=0):
    in_specs = (
        P(("rep", "fs", "tp"), None),
        P("fs", "tp"),
        P("fs", "tp"),
        P("tp", "fs"),
        P("fs", "tp"),
        P("fs", "tp"),
        P("fs", "tp"),
        P("fs", "tp"),
        P(),
        P(None, "tp"),
        P("tp"),
        P(),
        P("tp", "fs"),
        P(),
    )
    return jax.shard_map(
        functools.partial(on_device, stop),
        mesh=mesh,
        in_specs=in_specs,
        out_specs=P(("rep", "fs", "tp"), None),
        check_vma=False,
    )
```
